32 devices in a mesh: sp: 8 (over z, x), dp: 4 (over y, core).
Axes of the slice: x: 2, y: 2, z: 4, core: 2. Of those that a mesh axis runs over, the one named last changes fastest.
Arguments:
- queries: bfloat16 [16, 8, 512, 128], P('dp', None, 'sp'), may hold values from -6 to 6
- keys: bfloat16 [16, 8, 512, 128], P('dp', None, 'sp'), may hold values from -6 to 6
- values: bfloat16 [16, 8, 512, 128], P('dp', None, 'sp'), may hold values from -6 to 6
- input_gate: bfloat16 [16, 8, 512], P('dp', None, 'sp'), may hold values from -6 to 140
- forget_gate: bfloat16 [16, 8, 512], P('dp', None, 'sp'), may hold values from 0.5 to 11.5
- start_memory: float32 [16, 8, 128, 128], P('dp', None, 'sp'), may hold values from -6 to 6
- start_norm: float32 [16, 8, 128], P('dp', None, 'sp'), may hold values from -24 to 24
- start_level: float32 [16, 8], P('dp'), may hold values from 2 to 4
- head_gain: float32 [8, 128], replicated, may hold values from 0.1 to 1.9
- out_weight: bfloat16 [1024, 4096], P(None, 'dp'), may hold values from -0.1875 to 0.1875
Outputs:
- mixed: bfloat16 [16, 512, 4096], P('dp', 'sp')
The draws below stay inside these ranges and needn't reach their ends.
All inputs are finite; a program needn't handle non-finite values.
Results may differ from the reference program's by a relative error of at most 0.019.
Values may be sent and summed in bfloat16 or wider, within the bound.
A program may use at most 64 MiB of HBM per device.

```python
import jax
import jax.numpy as jnp
from jax import lax

D = 4096
HEADS = 8
HD = 128
BLOCK = 64
SEG = 64
MIX = 1024
LEN = 512
BATCH = 16


def draw_input_gate(key, part):
    first, second, third = jax.random.split(key, 3)
    plain = jax.random.normal(first, (BATCH, HEADS, LEN), jnp.float32)
    result = jnp.clip(plain, -6.0, 6.0)
    return result.astype(jnp.bfloat16)


def draw_forget_gate(key, part):
    first, second, third = jax.random.split(key, 3)
    slow_share = 0.5
    slow = jax.random.bernoulli(first, slow_share, (BATCH, HEADS, 1))
    base = jnp.where(slow, jnp.log(LEN / 1.2), 3.5)
    spans = LEN // SEG
    factor = jnp.exp(jax.random.uniform(second, (BATCH, HEADS, spans), jnp.float32, -0.693, 0.693))
    factor = jnp.repeat(factor, SEG, axis=2)
    noise = 0.3 * jax.random.normal(third, (BATCH, HEADS, LEN), jnp.float32)
    result = jnp.clip(base - jnp.log(factor) + noise, 0.5, 11.5)
    return result.astype(jnp.bfloat16)


def block_levels(rng, extent, pieces, low, top_value):
    level, own = 1.0, jax.random.fold_in(rng, 6)
    for dim, parts in pieces:
        steps = jnp.exp(jax.random.uniform(jax.random.fold_in(own, dim), (parts,), jnp.float32, low / len(pieces), top_value / len(pieces)))
        level = level * jnp.repeat(steps, extent[dim] // parts).reshape([-1 if axis == dim else 1 for axis in range(len(extent))])
    return level


def centred(key, shape, spread, bound, shards=(), kind=jnp.bfloat16):
    values = jax.random.normal(key, shape, jnp.float32) * spread
    if len(shards) > 0:
        values = block_levels(key, shape, shards, -0.22, 0.18) * values
    return jnp.clip(values, min=-bound, max=bound).astype(kind)


def setup_inputs(seed: int = 0) -> dict:
    seeds = jax.random.split(jax.random.key(seed), 11)
    queries = centred(seeds[0], (BATCH, HEADS, LEN, HD), 1.0, 6.0, ((0, 4), (2, 8)))
    keys = centred(seeds[1], (BATCH, HEADS, LEN, HD), 1.0, 6.0, ((0, 4), (2, 8)))
    values = centred(seeds[2], (BATCH, HEADS, LEN, HD), 1.0, 6.0, ((0, 4), (2, 8)))
    input_gate = draw_input_gate(jax.random.fold_in(seeds[10], 71), 0)
    forget_gate = draw_forget_gate(jax.random.fold_in(seeds[10], 71), 0)
    start_memory = centred(seeds[5], (BATCH, HEADS, HD, HD), 1.0, 6.0, ((0, 4), (2, 8)), jnp.float32)
    start_norm = centred(seeds[6], (BATCH, HEADS, HD), 4.0, 24.0, ((0, 4), (2, 8)), jnp.float32)
    start_level = jnp.clip(2.0 + 2.0 * jax.random.uniform(seeds[7], (BATCH, HEADS), jnp.float32) ** block_levels(seeds[7], (BATCH, HEADS), ((0, 4),), -0.2, 0.2), 2.0, 4.0)
    head_gain = jnp.clip(1.0 + 0.18 * jax.random.normal(seeds[8], (HEADS, HD), jnp.float32), 0.1, 1.9)
    out_weight = centred(seeds[9], (MIX, D), MIX ** -0.5, 0.1875, ((1, 4),))
    return dict(queries=queries, keys=keys, values=values, input_gate=input_gate, forget_gate=forget_gate, start_memory=start_memory, start_norm=start_norm, start_level=start_level, head_gain=head_gain, out_weight=out_weight)


negative_fill = -1e30
highest = lax.Precision.HIGHEST


def cell_scan(query, key_in, value, input_pre, forget_pre, memory, normal, stabilizer):
    item_count, length, head_width = query.shape
    blocks = length // BLOCK
    factor = head_width ** -0.5

    def blocked(tensor):
        return jnp.moveaxis(tensor.reshape((item_count, blocks, BLOCK) + tensor.shape[2:]), 1, 0)

    inputs = (blocked(query), blocked(key_in), blocked(value),
              blocked(input_pre.astype(jnp.float32)), blocked(jax.nn.log_sigmoid(forget_pre.astype(jnp.float32))))
    causal = jnp.tril(jnp.ones((BLOCK, BLOCK), dtype=bool))

    def advance(state, block_data):
        memory, normal, stabilizer = state
        query_block, key_block, value_block, gate_in, gate_keep = block_data
        query_wide = query_block.astype(jnp.float32)
        key_wide = key_block.astype(jnp.float32)
        value_wide = value_block.astype(jnp.float32)
        scaled = query_wide * factor
        cumulative = jnp.cumsum(gate_keep, axis=-1)
        logits = jnp.where(causal, cumulative[:, :, None] - cumulative[:, None, :] + gate_in[:, None, :], negative_fill)
        carried = cumulative + stabilizer[:, None]
        running_max = jnp.maximum(carried, jnp.max(logits, axis=-1))
        raw = jnp.einsum('ptd,psd->pts', query_wide, key_wide, precision=highest) * factor
        scores = raw * jnp.exp(logits - running_max[..., None])
        rounded = scores.astype(jnp.bfloat16).astype(jnp.float32)
        carry_weight = jnp.exp(carried - running_max)
        numerator = jnp.einsum('pts,pse->pte', rounded, value_wide, precision=highest) + carry_weight[..., None] * jnp.einsum('ptd,pde->pte', scaled, memory, precision=highest)
        denominator = jnp.sum(scores, axis=-1) + carry_weight * jnp.einsum('ptd,pd->pt', scaled, normal, precision=highest)
        output = numerator / jnp.maximum(jnp.abs(denominator), 1.0)[..., None]
        block_total = cumulative[:, -1]
        weights_log = block_total[:, None] - cumulative + gate_in
        stabilizer_new = jnp.maximum(block_total + stabilizer, jnp.max(weights_log, axis=-1))
        weights = jnp.exp(weights_log - stabilizer_new[:, None])
        shrink = jnp.exp(block_total + stabilizer - stabilizer_new)
        weighted = key_wide * weights[..., None]
        packed = weighted.astype(jnp.bfloat16).astype(jnp.float32)
        memory_new = shrink[:, None, None] * memory + jnp.einsum('psd,pse->pde', packed, value_wide, precision=highest)
        normal_new = shrink[:, None] * normal + jnp.sum(weighted, axis=1)
        return (memory_new, normal_new, stabilizer_new), output

    start = (memory.astype(jnp.float32), normal.astype(jnp.float32), stabilizer.astype(jnp.float32))
    _, outputs = lax.scan(advance, start, inputs)
    return jnp.moveaxis(outputs, 0, 1).reshape(item_count, length, head_width).astype(jnp.bfloat16)


def normalize(hidden, gain):
    entries = hidden.astype(jnp.float32)
    return (entries * gain[:, None, :]).astype(jnp.bfloat16)


def reference(queries, keys, values, input_gate, forget_gate, start_memory, start_norm, start_level, head_gain, out_weight):
    batch, heads, length, head_width = queries.shape
    count = batch * heads
    hidden = cell_scan(queries.reshape(count, length, head_width), keys.reshape(count, length, head_width),
                       values.reshape(count, length, head_width), input_gate.reshape(count, length),
                       forget_gate.reshape(count, length), start_memory.reshape(count, head_width, head_width),
                       start_norm.reshape(count, head_width), start_level.reshape(count))
    normed = normalize(hidden.reshape(batch, heads, length, head_width), head_gain)
    flat_rows = normed.transpose(0, 2, 1, 3).reshape(batch * length, heads * head_width)
    mixed = jnp.dot(flat_rows, out_weight, preferred_element_type=jnp.float32).astype(jnp.bfloat16)
    return mixed.reshape(batch, length, out_weight.shape[1])
```

```python
import jax
import jax.numpy as jnp
from jax import lax
from jax.experimental import pallas as pl
from jax.experimental.pallas import tpu as pltpu
from jax.sharding import PartitionSpec as P

MESH = pl.DeviceIdType.MESH
FILL = -1e30
PER = 2
HOP = 3
PIECES = 16
SKIP = 7
TAIL = 16


def layer_kernel(
    sizes,
    q_hbm,
    k_hbm,
    v_hbm,
    ig_hbm,
    fg_hbm,
    w_hbm,
    mem_ref,
    norm_ref,
    level_ref,
    gain_ref,
    out_ref,
    xq,
    xk,
    xv,
    igr,
    fgr,
    cast,
    mem_in,
    norm_in,
    norm_out,
    offs,
    peaks,
    starts,
    off_g,
    wrow,
    arow,
    srow,
    pcol,
    grown,
    st_in,
    st_out,
    act,
    back,
    weight,
    loc_sem,
    gate_send,
    gate_recv,
    x_send,
    x_recv,
    mem_send,
    mem_recv,
    st_send,
    st_recv,
    back_send,
    back_recv,
    wy_send,
    wy_recv,
    wz_send,
    wz_recv,
    wd_send,
    wd_recv,
    own_send,
    own_recv,
):
    n_sp, n_dp, seqs, heads, tokens, width, channels = sizes
    n_groups = n_sp // 2
    chips = n_dp // 2
    half = seqs // 2
    items = half * heads
    span = 2 * tokens
    chunks = items // PER
    per_seq = heads // PER
    rows = w_hbm.shape[0] // PIECES
    factor = width ** (-0.5)
    f32, bf16 = jnp.float32, jnp.bfloat16

    sp, dp = lax.axis_index("sp"), lax.axis_index("dp")
    g, m = sp // 2, sp % 2
    y, core = dp // 2, dp % 2
    mate = g * 2 + (1 - m)
    twin = y * 2 + (1 - core)
    even = 1 - g % 2

    def remote(src, dst, send, recv, to_sp, to_dp):
        return pltpu.make_async_remote_copy(
            src_ref=src,
            dst_ref=dst,
            send_sem=send,
            recv_sem=recv,
            device_id=(to_sp, to_dp),
            device_id_type=MESH,
        )

    mine = pl.ds(half * m, half)
    here = pl.ds(pl.multiple_of(m * tokens, tokens), tokens)
    local = [
        pltpu.make_async_copy(ig_hbm.at[mine], igr.at[sp], loc_sem.at[0]),
        pltpu.make_async_copy(fg_hbm.at[mine], fgr.at[sp], loc_sem.at[1]),
        pltpu.make_async_copy(k_hbm.at[mine], xk.at[:, :, here, :], loc_sem.at[2]),
        pltpu.make_async_copy(v_hbm.at[mine], xv.at[:, :, here, :], loc_sem.at[3]),
        pltpu.make_async_copy(q_hbm.at[mine], xq.at[:, :, here, :], loc_sem.at[4]),
        pltpu.make_async_copy(w_hbm, weight.at[dp], loc_sem.at[5]),
    ]
    for copy in local:
        copy.start()

    barrier = pltpu.get_barrier_semaphore()
    for d in range(1, n_sp):
        pl.semaphore_signal(barrier, inc=1, device_id=((sp + d) % n_sp, dp), device_id_type=MESH)
    pl.semaphore_signal(barrier, inc=1, device_id=(sp, twin), device_id_type=MESH)
    for j in range(1, chips):
        pl.semaphore_signal(
            barrier, inc=1, device_id=(sp, ((y + j) % chips) * 2 + core), device_id_type=MESH
        )
    cast[...] = mem_ref[...].astype(bf16)
    pl.semaphore_wait(barrier, n_sp - 1 + 1 + chips - 1)

    def gate_copy(d):
        to = (sp + d) % n_sp
        part = pl.ds(half * (to % 2), half)
        return [
            remote(ig_hbm.at[part], igr.at[sp], gate_send.at[0, d], gate_recv.at[0, d], to, dp),
            remote(fg_hbm.at[part], fgr.at[sp], gate_send.at[1, d], gate_recv.at[1, d], to, dp),
        ]

    def x_copy(kind, c):
        src, dst = ((k_hbm, xk), (v_hbm, xv), (q_hbm, xq))[kind]
        s, h = c // per_seq, (c % per_seq) * PER
        return remote(
            src.at[half * (1 - m) + s, pl.ds(h, PER)],
            dst.at[s, pl.ds(h, PER), here, :],
            x_send.at[kind, c],
            x_recv.at[kind, c],
            mate,
            dp,
        )

    def own_copy():
        return remote(w_hbm, weight.at[dp], own_send.at[0], own_recv.at[0], sp, twin)

    def piece(r):
        return pl.ds(pl.multiple_of(r * rows, rows), rows)

    direct = PIECES - SKIP

    def direct_piece(k):
        return jnp.where(k < SKIP, even * SKIP + k, k + SKIP)

    def wy_copy(j, k):
        r = piece(direct_piece(k))
        return remote(
            w_hbm.at[r],
            weight.at[dp, r],
            wy_send.at[j, k],
            wy_recv.at[j, k],
            sp,
            ((y + j) % chips) * 2 + core,
        )

    def wz_copy(j, k):
        shard = ((y - j + chips) % chips) * 2 + core
        r = piece(direct_piece(k))
        return remote(
            weight.at[shard, r],
            weight.at[shard, r],
            wz_send.at[j, k],
            wz_recv.at[j, k],
            ((g + n_groups - 1) % n_groups) * 2 + m,
            dp,
        )

    def wd_copy(j, r):
        shard = ((y - j + chips) % chips) * 2 + core
        return remote(
            weight.at[shard, piece(r)],
            weight.at[shard, piece(r)],
            wd_send.at[j, r],
            wd_recv.at[j, r],
            sp,
            twin,
        )

    for d in range(1, n_sp):
        for copy in gate_copy(d):
            copy.start()

    @pl.loop(0, chunks)
    def _(c):
        x_copy(0, c).start()
        x_copy(1, c).start()

    @pl.loop(0, direct)
    def _(k):
        for j in range(1, chips):
            wy_copy(j, k).start()

    def mem_copy(member):
        return [
            remote(
                cast.at[pl.ds(half * member, half)],
                mem_in.at[sp],
                mem_send.at[0, member],
                mem_recv.at[0, sp],
                member,
                dp,
            ),
            remote(
                norm_ref.at[pl.ds(half * member, half)],
                norm_in.at[sp],
                mem_send.at[1, member],
                mem_recv.at[1, sp],
                member,
                dp,
            ),
        ]

    def mem_arrived(d):
        return [
            remote(cast.at[mine], mem_in.at[d], mem_send.at[0, 0], mem_recv.at[0, d], d, dp),
            remote(norm_ref.at[mine], norm_in.at[d], mem_send.at[1, 0], mem_recv.at[1, d], d, dp),
        ]

    for member in range(2):

        @pl.when(sp != member)
        def _():
            for copy in mem_copy(member):
                copy.start()

    @pl.loop(0, chunks)
    def _(c):
        x_copy(2, c).start()

    own_copy().start()

    @pl.when(g == 0)
    def _():
        mem_in[sp] = cast[mine]
        norm_in[sp] = norm_ref[mine]

    local[0].wait()
    local[1].wait()
    for d in range(1, n_sp):
        for copy in gate_copy(d):
            copy.wait_recv()

    lane = lax.broadcasted_iota(jnp.int32, (n_groups * items, span), 1)

    def whole(ref):
        return jnp.concatenate(
            [
                jnp.concatenate(
                    [
                        ref[2 * i].astype(f32).reshape(items, tokens),
                        ref[2 * i + 1].astype(f32).reshape(items, tokens),
                    ],
                    axis=1,
                )
                for i in range(n_groups)
            ],
            axis=0,
        )

    gate_in = whole(igr)
    pre = whole(fgr)
    total = jnp.minimum(pre, 0.0) - jnp.log1p(jnp.exp(-jnp.abs(pre)))
    step = 1
    while step < span:
        total = total + jnp.where(lane >= step, pltpu.roll(total, step, 1), 0.0)
        step *= 2
    base = jnp.zeros((items, 1), f32)
    parts = []
    for i in range(n_groups):
        part = total[i * items : (i + 1) * items]
        parts.append(gate_in[i * items : (i + 1) * items] - (part + base))
        base = base + part[:, span - 1 : span]
    offset = jnp.concatenate(parts, axis=0)
    peak = offset
    step = 1
    while step < span:
        peak = jnp.maximum(peak, jnp.where(lane >= step, pltpu.roll(peak, step, 1), FILL))
        step *= 2
    level = level_ref[pl.ds(pl.multiple_of(items * m, items), items), :]
    for i in range(n_groups):
        part = peak[i * items : (i + 1) * items]
        starts[i] = level
        offs[i] = offset[i * items : (i + 1) * items]
        peaks[i] = jnp.maximum(part, level)
        level = jnp.maximum(level, jnp.broadcast_to(part[:, span - 1 : span], part.shape))
    starts[n_groups] = level
    first, last = starts[g], starts[g + 1]
    mine_off = offs[g]
    off_g[...] = mine_off
    wrow[...] = jnp.exp(mine_off - last)
    arow[...] = jnp.exp(first - last)
    srow[...] = first
    columns = jnp.transpose(peaks[g])
    for i in range(items):
        pcol[i] = jnp.broadcast_to(columns[:, i : i + 1], (span, span))

    for copy in local[2:5]:
        copy.wait()

    @pl.when(g == 0)
    def _():
        for d in range(n_sp):

            @pl.when(sp != d)
            def _():
                for copy in mem_arrived(d):
                    copy.wait_recv()

        norm = norm_in[0].reshape(items, width)
        for d in range(1, n_sp):
            norm = norm + norm_in[d].reshape(items, width)
        norm_out[...] = norm

        @pl.loop(0, chunks)
        def _(c):
            s, h = c // per_seq, (c % per_seq) * PER
            for p in range(PER):
                if channels % 16 == 0:
                    st_in[c, p * width : (p + 1) * width] = mem_in[:, s, h + p].reshape(
                        width, width
                    )
                else:
                    for d in range(n_sp):
                        grown[0, d * channels : (d + 1) * channels] = mem_in[d, s, h + p].astype(f32)
                    st_in[c, p * width : (p + 1) * width] = grown[0, 0:width].astype(bf16)
            row = lax.broadcasted_iota(jnp.int32, (TAIL, width), 0)
            tail = jnp.zeros((TAIL, width), f32)
            for p in range(PER):
                tail = jnp.where(row == p, norm_out[pl.ds(c * PER + p, 1), :], tail)
            st_in[c, PER * width :] = tail.astype(bf16)

    tail_row = lax.broadcasted_iota(jnp.int32, (TAIL, width), 0)

    def grow(c):
        x_copy(0, c).wait_recv()
        x_copy(1, c).wait_recv()
        s, h = c // per_seq, (c % per_seq) * PER
        tail = jnp.zeros((TAIL, width), f32)
        for p in range(PER):
            key, value = xk[s, h + p], xv[s, h + p]
            w = wrow[pl.ds(c * PER + p, 1), :]
            scaled = (jnp.transpose(key.astype(f32)) * w).astype(bf16)
            grown[c, p * width : (p + 1) * width] = jnp.dot(
                scaled, value, preferred_element_type=f32
            )
            high = w.astype(bf16).astype(f32)
            both = jnp.where(tail_row == 0, high, jnp.where(tail_row == 1, w - high, 0.0))
            norm = jnp.dot(both.astype(bf16), key, preferred_element_type=f32)
            norm = norm[0:1] + norm[1:2]
            tail = jnp.where(tail_row == p, norm, tail)
        grown[c, PER * width :] = tail

    def st_copy(c):
        return remote(
            st_out.at[c],
            st_in.at[c],
            st_send.at[c],
            st_recv.at[c],
            lax.rem(sp + 2, n_sp),
            dp,
        )

    def chain(c):
        @pl.when(g > 0)
        def _():
            st_copy(c).wait_recv()

        @pl.when(g < n_groups - 1)
        def _():
            tail = jnp.zeros((TAIL, width), f32)
            for p in range(PER):
                part = pl.ds(p * width, width)
                a = arow[pl.ds(c * PER + p, 1), :]
                st_out[c, part] = (st_in[c, part].astype(f32) * a + grown[c, part]).astype(bf16)
                tail = jnp.where(tail_row == p, a, tail)
            part = pl.ds(PER * width, TAIL)
            st_out[c, part] = (st_in[c, part].astype(f32) * tail + grown[c, part]).astype(bf16)
            st_copy(c).start()

    def back_copy(c):
        s, h = c // per_seq, (c % per_seq) * PER
        lanes = pl.ds(pl.multiple_of(h * width, PER * width), PER * width)
        return remote(
            back.at[s, :, lanes],
            act.at[half * m + s, :, lanes],
            back_send.at[c],
            back_recv.at[c],
            mate,
            dp,
        )

    def back_arrived(c):
        s, h = c // per_seq, (c % per_seq) * PER
        lanes = pl.ds(pl.multiple_of(h * width, PER * width), PER * width)
        return remote(
            back.at[s, :, lanes],
            act.at[half * (1 - m) + s, :, lanes],
            back_send.at[c],
            back_recv.at[c],
            mate,
            dp,
        )

    t_row = lax.broadcasted_iota(jnp.int32, (span, span), 0)
    s_col = lax.broadcasted_iota(jnp.int32, (span, span), 1)
    causal = s_col <= t_row
    ones = jnp.ones((span, width), bf16)

    def emit(c):
        x_copy(2, c).wait_recv()
        s, h = c // per_seq, (c % per_seq) * PER
        for p in range(PER):
            i = c * PER + p
            query, key, value = xq[s, h + p], xk[s, h + p], xv[s, h + p]
            memory = st_in[c, p * width : (p + 1) * width]
            norm = jnp.broadcast_to(
                st_in[c, PER * width :].astype(f32)[p : p + 1], (width, width)
            ).astype(bf16)
            raw = lax.dot_general(
                query,
                jnp.concatenate([key, norm], axis=0),
                (((1,), (1,)), ((), ())),
                preferred_element_type=f32,
            )
            column = pcol[i]
            gap = jnp.where(causal, off_g[pl.ds(i, 1), :] - column, FILL)
            scores = (raw[:, :span] * factor * jnp.exp(gap)).astype(bf16)
            weigh = jnp.exp(srow[pl.ds(i, 1), :] - column) * factor
            both = jnp.dot(
                scores, jnp.concatenate([value, ones], axis=1), preferred_element_type=f32
            )
            num = both[:, :width] + weigh * jnp.dot(query, memory, preferred_element_type=f32)
            den = both[:, width:] + weigh * raw[:, span:]
            hidden = (num / jnp.maximum(jnp.abs(den), 1.0)).astype(bf16)
            normed = (hidden.astype(f32) * gain_ref[pl.ds(h + p, 1), :]).astype(bf16)
            top, low = normed[:tokens], normed[tokens:]
            lanes = pl.ds(pl.multiple_of((h + p) * width, width), width)
            act[half * m + s, :, lanes] = jnp.where(m == 0, top, low)
            back[s, :, lanes] = jnp.where(m == 0, low, top)
        back_copy(c).start()

    out_slot = jnp.maximum(chunks, HOP * g)
    slots = max(
        chunks + max(chunks, HOP * (n_groups - 1)),
        2 * (direct - 1) + 2,
        2 * (SKIP - 1) + 7,
    )

    @pl.loop(0, slots)
    def _(t):
        @pl.when(t < chunks)
        def _():
            grow(t)

        c = t - HOP * g

        @pl.when((c >= 0) & (c < chunks))
        def _():
            chain(c)

        o = t - out_slot

        @pl.when((o >= 0) & (o < chunks))
        def _():
            emit(o)

        k = (t - 1) // 2

        @pl.when((t % 2 == 1) & (k < direct))
        def _():
            for j in range(1, chips):
                wy_copy(j, k).wait_recv()
                wd_copy(j, direct_piece(k)).start()

                @pl.when(k < SKIP)
                def _():
                    wz_copy(j, k).start()

        z = (t - 6) // 2

        @pl.when((t >= 6) & (t % 2 == 0) & (z < SKIP))
        def _():
            for j in range(1, chips):
                wz_copy(j, z).wait_recv()
                wd_copy(j, (1 - even) * SKIP + z).start()

    local[5].wait()
    own_copy().wait()
    for j in range(1, chips):

        @pl.loop(0, PIECES)
        def _(r):
            wd_copy(j, r).wait()

    @pl.loop(0, chunks)
    def _(c):
        back_arrived(c).wait_recv()

    left = act[...].reshape(seqs * tokens, heads * width)
    columns_each = weight.shape[2]
    tile = min(512, columns_each)
    tiles = columns_each // tile

    @pl.loop(0, n_dp * tiles)
    def _(n):
        j, b = n // tiles, n % tiles
        shard = (dp + j) % n_dp
        at = pl.ds(pl.multiple_of(b * tile, tile), tile)
        product = jnp.dot(left, weight[shard, :, at], preferred_element_type=f32).astype(bf16)
        out_ref[:, :, pl.ds(pl.multiple_of(shard * columns_each + b * tile, tile), tile)] = (
            product.reshape(seqs, tokens, tile)
        )

    for d in range(1, n_sp):
        for copy in gate_copy(d):
            copy.wait_send()

    @pl.loop(0, chunks)
    def _(c):
        for kind in range(3):
            x_copy(kind, c).wait_send()
        back_copy(c).wait_send()

        @pl.when(g < n_groups - 1)
        def _():
            st_copy(c).wait_send()

    for member in range(2):

        @pl.when(sp != member)
        def _():
            for copy in mem_copy(member):
                copy.wait_send()

    @pl.loop(0, direct)
    def _(k):
        for j in range(1, chips):
            wy_copy(j, k).wait_send()

            @pl.when(k < SKIP)
            def _():
                wz_copy(j, k).wait_send()


def on_device(
    queries,
    keys,
    values,
    input_gate,
    forget_gate,
    start_memory,
    start_norm,
    start_level,
    head_gain,
    out_weight,
):
    seqs, heads, tokens, width = queries.shape
    n_sp, n_dp = lax.axis_size("sp"), lax.axis_size("dp")
    channels = start_memory.shape[2]
    mix, columns = out_weight.shape
    half = seqs // 2
    items = half * heads
    span = 2 * tokens
    groups = n_sp // 2
    chips = n_dp // 2
    chunks = items // PER
    direct = PIECES - SKIP
    f32, bf16 = jnp.float32, jnp.bfloat16
    level = jnp.broadcast_to(start_level.reshape(seqs * heads, 1), (seqs * heads, span))
    place = lax.axis_index("sp") * channels
    norm = lax.dynamic_update_slice(
        jnp.zeros((seqs, heads, width), f32), start_norm, (0, 0, place)
    )
    sizes = (n_sp, n_dp, seqs, heads, tokens, width, channels)
    any_spec = pl.BlockSpec(memory_space=pl.ANY)
    vmem = pl.BlockSpec(memory_space=pltpu.VMEM)
    dma = pltpu.SemaphoreType.DMA
    return pl.pallas_call(
        lambda *refs: layer_kernel(sizes, *refs),
        out_shape=jax.ShapeDtypeStruct((seqs, tokens, n_dp * columns), bf16),
        in_specs=[any_spec] * 6 + [vmem] * 4,
        out_specs=vmem,
        scratch_shapes=[
            pltpu.VMEM((half, heads, span, width), bf16),
            pltpu.VMEM((half, heads, span, width), bf16),
            pltpu.VMEM((half, heads, span, width), bf16),
            pltpu.VMEM((n_sp, half, heads, tokens), bf16),
            pltpu.VMEM((n_sp, half, heads, tokens), bf16),
            pltpu.VMEM((seqs, heads, channels, width), bf16),
            pltpu.VMEM((n_sp, half, heads, channels, width), bf16),
            pltpu.VMEM((n_sp, half, heads, width), f32),
            pltpu.VMEM((items, width), f32),
            pltpu.VMEM((groups, items, span), f32),
            pltpu.VMEM((groups, items, span), f32),
            pltpu.VMEM((groups + 1, items, span), f32),
            pltpu.VMEM((items, span), f32),
            pltpu.VMEM((items, span), f32),
            pltpu.VMEM((items, span), f32),
            pltpu.VMEM((items, span), f32),
            pltpu.VMEM((items, span, span), f32),
            pltpu.VMEM((chunks, PER * width + TAIL, width), f32),
            pltpu.VMEM((chunks, PER * width + TAIL, width), bf16),
            pltpu.VMEM((chunks, PER * width + TAIL, width), bf16),
            pltpu.VMEM((seqs, tokens, heads * width), bf16),
            pltpu.VMEM((half, tokens, heads * width), bf16),
            pltpu.VMEM((n_dp, mix, columns), bf16),
            dma((6,)),
            dma((2, n_sp)),
            dma((2, n_sp)),
            dma((3, chunks)),
            dma((3, chunks)),
            dma((2, 2)),
            dma((2, n_sp)),
            dma((chunks,)),
            dma((chunks,)),
            dma((chunks,)),
            dma((chunks,)),
            dma((chips, direct)),
            dma((chips, direct)),
            dma((chips, SKIP)),
            dma((chips, SKIP)),
            dma((chips, PIECES)),
            dma((chips, PIECES)),
            dma((1,)),
            dma((1,)),
        ],
        compiler_params=pltpu.CompilerParams(
            collective_id=0, has_side_effects=True, vmem_limit_bytes=40 * 1024 * 1024
        ),
        name="layer",
    )(
        queries,
        keys,
        values,
        input_gate,
        forget_gate,
        out_weight,
        start_memory,
        norm,
        level,
        head_gain,
    )


def solution(mesh):
    in_specs = (
        P("dp", None, "sp", None),
        P("dp", None, "sp", None),
        P("dp", None, "sp", None),
        P("dp", None, "sp"),
        P("dp", None, "sp"),
        P("dp", None, "sp", None),
        P("dp", None, "sp"),
        P("dp", None),
        P(),
        P(None, "dp"),
    )
    out_specs = P("dp", "sp", None)
    return jax.shard_map(
        on_device, mesh=mesh, in_specs=in_specs, out_specs=out_specs, check_vma=False
    )
```

```python
import jax
import jax.numpy as jnp
from jax import lax
from jax.experimental import pallas as pl
from jax.experimental.pallas import tpu as pltpu
from jax.sharding import PartitionSpec as P

MESH = pl.DeviceIdType.MESH
FILL = -1e30
PER = 2
HOP = 3
PIECES = 16
SKIP = 6
TAIL = 16


def layer_kernel(
    sizes,
    q_hbm,
    k_hbm,
    v_hbm,
    ig_hbm,
    fg_hbm,
    w_hbm,
    mem_hbm,
    norm_hbm,
    level_hbm,
    gain_hbm,
    out_ref,
    mem_ref,
    norm_raw,
    level_ref,
    gain_ref,
    norm_ref,
    xq,
    xk,
    xv,
    igr,
    fgr,
    cast,
    mem_in,
    norm_in,
    norm_out,
    whole_ref,
    offs,
    peaks,
    starts,
    off_g,
    wrow,
    arow,
    srow,
    pcol,
    grown,
    st_in,
    st_out,
    act,
    back,
    weight,
    loc_sem,
    gate_send,
    gate_recv,
    x_send,
    x_recv,
    mem_send,
    mem_recv,
    norm_send,
    norm_recv,
    st_send,
    st_recv,
    back_send,
    back_recv,
    wy_send,
    wy_recv,
    wz_send,
    wu_send,
    wz_recv,
    wd_send,
    wd_recv,
    own_send,
    own_recv,
):
    n_sp, n_dp, seqs, heads, tokens, width, channels = sizes
    n_groups = n_sp // 2
    chips = n_dp // 2
    half = seqs // 2
    items = half * heads
    span = 2 * tokens
    chunks = items // PER
    per_seq = heads // PER
    rows = w_hbm.shape[0] // PIECES
    factor = width ** (-0.5)
    f32, bf16 = jnp.float32, jnp.bfloat16

    sp, dp = lax.axis_index("sp"), lax.axis_index("dp")
    g, m = sp // 2, sp % 2
    y, core = dp // 2, dp % 2
    mate = g * 2 + (1 - m)
    twin = y * 2 + (1 - core)
    even = 1 - g % 2

    def remote(src, dst, send, recv, to_sp, to_dp):
        return pltpu.make_async_remote_copy(
            src_ref=src,
            dst_ref=dst,
            send_sem=send,
            recv_sem=recv,
            device_id=(to_sp, to_dp),
            device_id_type=MESH,
        )

    mine = pl.ds(half * m, half)
    here = pl.ds(pl.multiple_of(m * tokens, tokens), tokens)
    local = [
        pltpu.make_async_copy(ig_hbm.at[mine], igr.at[sp], loc_sem.at[0]),
        pltpu.make_async_copy(fg_hbm.at[mine], fgr.at[sp], loc_sem.at[1]),
        pltpu.make_async_copy(k_hbm.at[mine], xk.at[:, :, here, :], loc_sem.at[2]),
        pltpu.make_async_copy(v_hbm.at[mine], xv.at[:, :, here, :], loc_sem.at[3]),
        pltpu.make_async_copy(q_hbm.at[mine], xq.at[:, :, here, :], loc_sem.at[4]),
        pltpu.make_async_copy(mem_hbm, mem_ref, loc_sem.at[5]),
        pltpu.make_async_copy(norm_hbm, norm_raw, loc_sem.at[6]),
        pltpu.make_async_copy(level_hbm, level_ref, loc_sem.at[7]),
        pltpu.make_async_copy(gain_hbm, gain_ref, loc_sem.at[8]),
        pltpu.make_async_copy(w_hbm, weight.at[dp], loc_sem.at[9]),
    ]
    for copy in local:
        copy.start()

    barrier = pltpu.get_barrier_semaphore()
    for d in range(1, n_sp):
        pl.semaphore_signal(barrier, inc=1, device_id=((sp + d) % n_sp, dp), device_id_type=MESH)
    pl.semaphore_signal(barrier, inc=1, device_id=(sp, twin), device_id_type=MESH)
    for j in range(1, chips):
        pl.semaphore_signal(
            barrier, inc=1, device_id=(sp, ((y + j) % chips) * 2 + core), device_id_type=MESH
        )
    local[5].wait()
    cast[...] = mem_ref[...].astype(bf16)
    local[6].wait()
    norm_ref[...] = jnp.zeros((seqs, heads, width), f32)
    norm_ref[:, :, 0:channels] = norm_raw[...]
    norm_ref[...] = pltpu.roll(
        norm_ref[...].reshape(seqs * heads, width), sp * channels, 1
    ).reshape(seqs, heads, width)
    pl.semaphore_wait(barrier, n_sp - 1 + 1 + chips - 1)

    def gate_copy(d):
        to = (sp + d) % n_sp
        part = pl.ds(half * (to % 2), half)
        return [
            remote(ig_hbm.at[part], igr.at[sp], gate_send.at[0, d], gate_recv.at[0, d], to, dp),
            remote(fg_hbm.at[part], fgr.at[sp], gate_send.at[1, d], gate_recv.at[1, d], to, dp),
        ]

    def x_copy(kind, c):
        src, dst = ((k_hbm, xk), (v_hbm, xv), (q_hbm, xq))[kind]
        s, h = c // per_seq, (c % per_seq) * PER
        return remote(
            src.at[half * (1 - m) + s, pl.ds(h, PER)],
            dst.at[s, pl.ds(h, PER), here, :],
            x_send.at[kind, c],
            x_recv.at[kind, c],
            mate,
            dp,
        )

    def own_copy():
        return remote(w_hbm, weight.at[dp], own_send.at[0], own_recv.at[0], sp, twin)

    def piece(r):
        return pl.ds(pl.multiple_of(r * rows, rows), rows)

    direct = PIECES - SKIP

    def direct_piece(k):
        return jnp.where(k < SKIP, even * SKIP + k, k + SKIP)

    def wy_copy(j, k):
        r = piece(direct_piece(k))
        return remote(
            w_hbm.at[r],
            weight.at[dp, r],
            wy_send.at[j, k],
            wy_recv.at[j, k],
            sp,
            ((y + j) % chips) * 2 + core,
        )

    def wz_copy(j, k, down=True):
        shard = ((y - j + chips) % chips) * 2 + core
        r = piece(direct_piece(k))
        to = lax.rem(sp + n_sp - 2, n_sp) if down else lax.rem(sp + 2, n_sp)
        return remote(
            weight.at[shard, r],
            weight.at[shard, r],
            (wz_send if down else wu_send).at[j, k],
            wz_recv.at[j, k],
            to,
            dp,
        )

    def wz_each(j, k, act):
        @pl.when(g > 0)
        def _():
            act(wz_copy(j, k))

        @pl.when(g == n_groups - 2)
        def _():
            act(wz_copy(j, k, down=False))

    def wd_copy(j, r):
        shard = ((y - j + chips) % chips) * 2 + core
        return remote(
            weight.at[shard, piece(r)],
            weight.at[shard, piece(r)],
            wd_send.at[j, r],
            wd_recv.at[j, r],
            sp,
            twin,
        )

    for d in range(1, n_sp):
        for copy in gate_copy(d):
            copy.start()

    def mem_copy(member, c):
        s, h = c // per_seq, (c % per_seq) * PER
        return remote(
            cast.at[half * member + s, pl.ds(h, PER)],
            mem_in.at[sp, s, pl.ds(h, PER)],
            mem_send.at[member, c],
            mem_recv.at[sp, c],
            member,
            dp,
        )

    def mem_arrived(d, c):
        s, h = c // per_seq, (c % per_seq) * PER
        return remote(
            cast.at[half * m + s, pl.ds(h, PER)],
            mem_in.at[d, s, pl.ds(h, PER)],
            mem_send.at[0, c],
            mem_recv.at[d, c],
            d,
            dp,
        )

    def norm_copy(member):
        return remote(
            norm_ref.at[pl.ds(half * member, half)],
            norm_in.at[sp],
            norm_send.at[member],
            norm_recv.at[sp],
            member,
            dp,
        )

    def norm_arrived(d):
        return remote(
            norm_ref.at[mine], norm_in.at[d], norm_send.at[0], norm_recv.at[d], d, dp
        )

    for member in range(2):

        @pl.when(sp != member)
        def _():
            norm_copy(member).start()

    @pl.loop(0, chunks)
    def _(c):
        for member in range(2):

            @pl.when(sp != member)
            def _():
                mem_copy(member, c).start()

    @pl.loop(0, chunks)
    def _(c):
        x_copy(0, c).start()
        x_copy(1, c).start()

    @pl.loop(0, direct)
    def _(k):
        for j in range(1, chips):
            wy_copy(j, k).start()

    @pl.loop(0, chunks)
    def _(c):
        x_copy(2, c).start()

    own_copy().start()

    @pl.when(g == 0)
    def _():
        mem_in[sp] = cast[mine]
        norm_in[sp] = norm_ref[mine]

    local[0].wait()
    local[1].wait()
    for d in range(1, n_sp):
        for copy in gate_copy(d):
            copy.wait_recv()

    lane = lax.broadcasted_iota(jnp.int32, (n_groups * items, span), 1)

    def whole(ref):
        return jnp.concatenate(
            [
                jnp.concatenate(
                    [
                        ref[2 * i].astype(f32).reshape(items, tokens),
                        ref[2 * i + 1].astype(f32).reshape(items, tokens),
                    ],
                    axis=1,
                )
                for i in range(n_groups)
            ],
            axis=0,
        )

    gate_in = whole(igr)
    pre = whole(fgr)
    total = jnp.minimum(pre, 0.0) - jnp.log1p(jnp.exp(-jnp.abs(pre)))
    step = 1
    while step < span:
        total = total + jnp.where(lane >= step, pltpu.roll(total, step, 1), 0.0)
        step *= 2
    base = jnp.zeros((items, 1), f32)
    parts = []
    for i in range(n_groups):
        part = total[i * items : (i + 1) * items]
        parts.append(gate_in[i * items : (i + 1) * items] - (part + base))
        base = base + part[:, span - 1 : span]
    offset = jnp.concatenate(parts, axis=0)
    peak = offset
    step = 1
    while step < span:
        peak = jnp.maximum(peak, jnp.where(lane >= step, pltpu.roll(peak, step, 1), FILL))
        step *= 2
    local[7].wait()
    local[8].wait()
    eye = lax.broadcasted_iota(jnp.int32, (heads, heads), 0) == lax.broadcasted_iota(
        jnp.int32, (heads, heads), 1
    )
    level = jnp.concatenate(
        [
            jnp.sum(
                jnp.where(eye, level_ref[pl.ds(half * m + i, 1), :], 0.0), axis=1, keepdims=True
            )
            for i in range(half)
        ],
        axis=0,
    )
    level = jnp.broadcast_to(level, (items, span))
    for i in range(n_groups):
        part = peak[i * items : (i + 1) * items]
        starts[i] = level
        offs[i] = offset[i * items : (i + 1) * items]
        peaks[i] = jnp.maximum(part, level)
        level = jnp.maximum(level, jnp.broadcast_to(part[:, span - 1 : span], part.shape))
    starts[n_groups] = level
    first, last = starts[g], starts[g + 1]
    mine_off = offs[g]
    off_g[...] = mine_off
    wrow[...] = jnp.exp(mine_off - last)
    arow[...] = jnp.exp(first - last)
    srow[...] = first
    columns = jnp.transpose(peaks[g])
    for i in range(items):
        pcol[i] = jnp.broadcast_to(columns[:, i : i + 1], (span, span))

    for copy in local[2:5]:
        copy.wait()

    tail_row = lax.broadcasted_iota(jnp.int32, (TAIL, width), 0)

    def grow(c):
        x_copy(0, c).wait_recv()
        x_copy(1, c).wait_recv()
        s, h = c // per_seq, (c % per_seq) * PER
        tail = jnp.zeros((TAIL, width), f32)
        for p in range(PER):
            key, value = xk[s, h + p], xv[s, h + p]
            w = wrow[pl.ds(c * PER + p, 1), :]
            scaled = (jnp.transpose(key.astype(f32)) * w).astype(bf16)
            grown[c, p * width : (p + 1) * width] = jnp.dot(
                scaled, value, preferred_element_type=f32
            )
            high = w.astype(bf16).astype(f32)
            both = jnp.where(tail_row == 0, high, jnp.where(tail_row == 1, w - high, 0.0))
            norm = jnp.dot(both.astype(bf16), key, preferred_element_type=f32)
            norm = norm[0:1] + norm[1:2]
            tail = jnp.where(tail_row == p, norm, tail)
        grown[c, PER * width :] = tail

    def st_copy(c):
        return remote(
            st_out.at[c],
            st_in.at[c],
            st_send.at[c],
            st_recv.at[c],
            lax.rem(sp + 2, n_sp),
            dp,
        )

    def seed(c):
        for d in range(n_sp):

            @pl.when(sp != d)
            def _():
                mem_arrived(d, c).wait_recv()

        @pl.when(c == 0)
        def _():
            for d in range(n_sp):

                @pl.when(sp != d)
                def _():
                    norm_arrived(d).wait_recv()

            norm = norm_in[0].reshape(items, width)
            for d in range(1, n_sp):
                norm = norm + norm_in[d].reshape(items, width)
            norm_out[...] = norm

        s, h = c // per_seq, (c % per_seq) * PER
        tail = jnp.zeros((TAIL, width), f32)
        for p in range(PER):
            if channels % 16 == 0:
                st_in[c, p * width : (p + 1) * width] = mem_in[:, s, h + p].reshape(width, width)
            else:
                for d in range(n_sp):
                    whole_ref[d * channels : (d + 1) * channels] = mem_in[d, s, h + p].astype(f32)
                st_in[c, p * width : (p + 1) * width] = whole_ref[...].astype(bf16)
            tail = jnp.where(tail_row == p, norm_out[pl.ds(c * PER + p, 1), :], tail)
        st_in[c, PER * width :] = tail.astype(bf16)

    def chain(c):
        @pl.when(g == 0)
        def _():
            seed(c)

        @pl.when(g > 0)
        def _():
            st_copy(c).wait_recv()

        @pl.when(g < n_groups - 1)
        def _():
            tail = jnp.zeros((TAIL, width), f32)
            for p in range(PER):
                part = pl.ds(p * width, width)
                a = arow[pl.ds(c * PER + p, 1), :]
                st_out[c, part] = (st_in[c, part].astype(f32) * a + grown[c, part]).astype(bf16)
                tail = jnp.where(tail_row == p, a, tail)
            part = pl.ds(PER * width, TAIL)
            st_out[c, part] = (st_in[c, part].astype(f32) * tail + grown[c, part]).astype(bf16)
            st_copy(c).start()

    def back_copy(c):
        s, h = c // per_seq, (c % per_seq) * PER
        lanes = pl.ds(pl.multiple_of(h * width, PER * width), PER * width)
        return remote(
            back.at[s, :, lanes],
            act.at[half * m + s, :, lanes],
            back_send.at[c],
            back_recv.at[c],
            mate,
            dp,
        )

    def back_arrived(c):
        s, h = c // per_seq, (c % per_seq) * PER
        lanes = pl.ds(pl.multiple_of(h * width, PER * width), PER * width)
        return remote(
            back.at[s, :, lanes],
            act.at[half * (1 - m) + s, :, lanes],
            back_send.at[c],
            back_recv.at[c],
            mate,
            dp,
        )

    t_row = lax.broadcasted_iota(jnp.int32, (span, span), 0)
    s_col = lax.broadcasted_iota(jnp.int32, (span, span), 1)
    causal = s_col <= t_row
    ones = jnp.ones((span, width), bf16)

    def emit(c):
        x_copy(2, c).wait_recv()
        s, h = c // per_seq, (c % per_seq) * PER
        for p in range(PER):
            i = c * PER + p
            query, key, value = xq[s, h + p], xk[s, h + p], xv[s, h + p]
            memory = st_in[c, p * width : (p + 1) * width]
            norm = jnp.broadcast_to(
                st_in[c, PER * width :].astype(f32)[p : p + 1], (width, width)
            ).astype(bf16)
            raw = lax.dot_general(
                query,
                jnp.concatenate([key, norm], axis=0),
                (((1,), (1,)), ((), ())),
                preferred_element_type=f32,
            )
            column = pcol[i]
            gap = jnp.where(causal, off_g[pl.ds(i, 1), :] - column, FILL)
            scores = (raw[:, :span] * factor * jnp.exp(gap)).astype(bf16)
            weigh = jnp.exp(srow[pl.ds(i, 1), :] - column) * factor
            both = jnp.dot(
                scores, jnp.concatenate([value, ones], axis=1), preferred_element_type=f32
            )
            num = both[:, :width] + weigh * jnp.dot(query, memory, preferred_element_type=f32)
            den = both[:, width:] + weigh * raw[:, span:]
            hidden = (num / jnp.maximum(jnp.abs(den), 1.0)).astype(bf16)
            normed = (hidden.astype(f32) * gain_ref[pl.ds(h + p, 1), :]).astype(bf16)
            top, low = normed[:tokens], normed[tokens:]
            lanes = pl.ds(pl.multiple_of((h + p) * width, width), width)
            act[half * m + s, :, lanes] = jnp.where(m == 0, top, low)
            back[s, :, lanes] = jnp.where(m == 0, low, top)
        back_copy(c).start()

    out_slot = jnp.maximum(chunks, HOP * g)
    slots = max(chunks + max(chunks, HOP * (n_groups - 1)), 2 * SKIP)

    def pass_on(j, k):
        wy_copy(j, k).wait_recv()
        wd_copy(j, direct_piece(k)).start()

    @pl.loop(0, slots)
    def _(t):
        @pl.when(t < chunks)
        def _():
            grow(t)

        c = t - HOP * g

        @pl.when((c >= 0) & (c < chunks))
        def _():
            chain(c)

        k = (t - 1) // 2

        @pl.when((t % 2 == 1) & (k < SKIP))
        def _():
            for j in range(1, chips):
                pass_on(j, k)
                wz_each(j, k, lambda copy: copy.start())

        o = t - out_slot

        @pl.when((o >= 0) & (o < chunks))
        def _():
            emit(o)

    def pass_up_to(first, last):
        @pl.loop(first, last)
        def _(k):
            for j in range(1, chips):
                pass_on(j, k)

    @pl.loop(0, SKIP)
    def _(k):
        for j in range(1, chips):
            wz_copy(j, k).wait_recv()
            wd_copy(j, (1 - even) * SKIP + k).start()

    middle = (SKIP + direct) // 2
    pass_up_to(SKIP, middle)

    @pl.loop(0, chunks)
    def _(c):
        back_arrived(c).wait_recv()

    left = act[...].reshape(seqs * tokens, heads * width)
    columns_each = weight.shape[2]
    tile = min(512, columns_each)
    tiles = columns_each // tile

    def project(shard):
        @pl.loop(0, tiles)
        def _(b):
            at = pl.ds(pl.multiple_of(b * tile, tile), tile)
            product = jnp.dot(left, weight[shard, :, at], preferred_element_type=f32)
            out_ref[:, :, pl.ds(pl.multiple_of(shard * columns_each + b * tile, tile), tile)] = (
                product.astype(bf16).reshape(seqs, tokens, tile)
            )

    local[9].wait()
    project(dp)
    own_copy().wait()
    project(twin)
    pass_up_to(middle, direct)
    for j in range(1, chips):
        project(((y - j + chips) % chips) * 2 + core)

        @pl.loop(0, PIECES)
        def _(r):
            wd_copy(j, r).wait()

        project(((y - j + chips) % chips) * 2 + 1 - core)

    for d in range(1, n_sp):
        for copy in gate_copy(d):
            copy.wait_send()

    @pl.loop(0, chunks)
    def _(c):
        for kind in range(3):
            x_copy(kind, c).wait_send()
        back_copy(c).wait_send()

        @pl.when(g < n_groups - 1)
        def _():
            st_copy(c).wait_send()

    for member in range(2):

        @pl.when(sp != member)
        def _():
            norm_copy(member).wait_send()

            @pl.loop(0, chunks)
            def _(c):
                mem_copy(member, c).wait_send()

    @pl.loop(0, direct)
    def _(k):
        for j in range(1, chips):
            wy_copy(j, k).wait_send()

            @pl.when(k < SKIP)
            def _():
                wz_each(j, k, lambda copy: copy.wait_send())


def on_device(
    queries,
    keys,
    values,
    input_gate,
    forget_gate,
    start_memory,
    start_norm,
    start_level,
    head_gain,
    out_weight,
):
    seqs, heads, tokens, width = queries.shape
    n_sp, n_dp = lax.axis_size("sp"), lax.axis_size("dp")
    channels = start_memory.shape[2]
    mix, columns = out_weight.shape
    half = seqs // 2
    items = half * heads
    span = 2 * tokens
    groups = n_sp // 2
    chips = n_dp // 2
    chunks = items // PER
    direct = PIECES - SKIP
    f32, bf16 = jnp.float32, jnp.bfloat16
    sizes = (n_sp, n_dp, seqs, heads, tokens, width, channels)
    operands = [
        pltpu.with_memory_space_constraint(array, pltpu.HBM)
        for array in (
            queries,
            keys,
            values,
            input_gate,
            forget_gate,
            out_weight,
            start_memory,
            start_norm,
            start_level,
            head_gain,
        )
    ]
    hbm_spec = pl.BlockSpec(memory_space=pltpu.HBM)
    vmem = pl.BlockSpec(memory_space=pltpu.VMEM)
    dma = pltpu.SemaphoreType.DMA
    return pl.pallas_call(
        lambda *refs: layer_kernel(sizes, *refs),
        out_shape=jax.ShapeDtypeStruct((seqs, tokens, n_dp * columns), bf16),
        in_specs=[hbm_spec] * len(operands),
        out_specs=vmem,
        scratch_shapes=[
            pltpu.VMEM((seqs, heads, channels, width), f32),
            pltpu.VMEM((seqs, heads, channels), f32),
            pltpu.VMEM((seqs, heads), f32),
            pltpu.VMEM((heads, width), f32),
            pltpu.VMEM((seqs, heads, width), f32),
            pltpu.VMEM((half, heads, span, width), bf16),
            pltpu.VMEM((half, heads, span, width), bf16),
            pltpu.VMEM((half, heads, span, width), bf16),
            pltpu.VMEM((n_sp, half, heads, tokens), bf16),
            pltpu.VMEM((n_sp, half, heads, tokens), bf16),
            pltpu.VMEM((seqs, heads, channels, width), bf16),
            pltpu.VMEM((n_sp, half, heads, channels, width), bf16),
            pltpu.VMEM((n_sp, half, heads, width), f32),
            pltpu.VMEM((items, width), f32),
            pltpu.VMEM((width, width), f32),
            pltpu.VMEM((groups, items, span), f32),
            pltpu.VMEM((groups, items, span), f32),
            pltpu.VMEM((groups + 1, items, span), f32),
            pltpu.VMEM((items, span), f32),
            pltpu.VMEM((items, span), f32),
            pltpu.VMEM((items, span), f32),
            pltpu.VMEM((items, span), f32),
            pltpu.VMEM((items, span, span), f32),
            pltpu.VMEM((chunks, PER * width + TAIL, width), f32),
            pltpu.VMEM((chunks, PER * width + TAIL, width), bf16),
            pltpu.VMEM((chunks, PER * width + TAIL, width), bf16),
            pltpu.VMEM((seqs, tokens, heads * width), bf16),
            pltpu.VMEM((half, tokens, heads * width), bf16),
            pltpu.VMEM((n_dp, mix, columns), bf16),
            dma((10,)),
            dma((2, n_sp)),
            dma((2, n_sp)),
            dma((3, chunks)),
            dma((3, chunks)),
            dma((2, chunks)),
            dma((n_sp, chunks)),
            dma((2,)),
            dma((n_sp,)),
            dma((chunks,)),
            dma((chunks,)),
            dma((chunks,)),
            dma((chunks,)),
            dma((chips, direct)),
            dma((chips, direct)),
            dma((chips, SKIP)),
            dma((chips, SKIP)),
            dma((chips, SKIP)),
            dma((chips, PIECES)),
            dma((chips, PIECES)),
            dma((1,)),
            dma((1,)),
        ],
        compiler_params=pltpu.CompilerParams(
            collective_id=0, has_side_effects=True, vmem_limit_bytes=40 * 1024 * 1024
        ),
        name="layer",
    )(*operands)


def solution(mesh):
    in_specs = (
        P("dp", None, "sp", None),
        P("dp", None, "sp", None),
        P("dp", None, "sp", None),
        P("dp", None, "sp"),
        P("dp", None, "sp"),
        P("dp", None, "sp", None),
        P("dp", None, "sp"),
        P("dp", None),
        P(),
        P(None, "dp"),
    )
    out_specs = P("dp", "sp", None)
    return jax.shard_map(
        on_device, mesh=mesh, in_specs=in_specs, out_specs=out_specs, check_vma=False
    )
```

```python
import jax
import jax.numpy as jnp
from jax import lax
from jax.experimental import pallas as pl
from jax.experimental.pallas import tpu as pltpu
from jax.sharding import PartitionSpec as P

MESH = pl.DeviceIdType.MESH
FILL = -1e30
PER = 2
HOP = 3
PIECES = 16
SKIP = 5
SIDE = 2
WHEN = (0, 1, 3, 4, 6, 8, 10, 12, 14)
LATE = (8, 8, 8, 8, 10, 12, 15, 16, 16)
WHEN_SKIP = 13
WHEN_SIDE = 15
OWN_SLOTS = 3
WHEN_OWN = 14
TAIL = 16


def layer_kernel(
    sizes,
    q_hbm,
    k_hbm,
    v_hbm,
    ig_hbm,
    fg_hbm,
    w_hbm,
    mem_hbm,
    norm_hbm,
    level_hbm,
    gain_hbm,
    out_ref,
    mem_ref,
    norm_raw,
    level_ref,
    gain_ref,
    norm_ref,
    xq,
    xk,
    xv,
    igr,
    fgr,
    cast,
    mem_in,
    norm_in,
    norm_out,
    whole_ref,
    offs,
    peaks,
    starts,
    off_g,
    wrow,
    arow,
    srow,
    pcol,
    grown,
    st_in,
    st_out,
    act,
    back,
    weight,
    loc_sem,
    gate_send,
    gate_recv,
    x_send,
    x_recv,
    mem_send,
    cross_recv,
    mem_recv,
    norm_send,
    norm_recv,
    st_send,
    st_recv,
    back_send,
    back_recv,
    wy_send,
    wy_recv,
    wz_send,
    wu_send,
    wz_recv,
    wx_send,
    wx_recv,
    wd_send,
    wd_recv,
    own_send,
    own_recv,
):
    n_sp, n_dp, seqs, heads, tokens, width, channels = sizes
    n_groups = n_sp // 2
    chips = n_dp // 2
    half = seqs // 2
    items = half * heads
    span = 2 * tokens
    chunks = items // PER
    per_seq = heads // PER
    rows = w_hbm.shape[0] // PIECES
    factor = width ** (-0.5)
    f32, bf16 = jnp.float32, jnp.bfloat16

    sp, dp = lax.axis_index("sp"), lax.axis_index("dp")
    g, m = sp // 2, sp % 2
    y, core = dp // 2, dp % 2
    mate = g * 2 + (1 - m)
    twin = y * 2 + (1 - core)
    even = 1 - g % 2

    def remote(src, dst, send, recv, to_sp, to_dp):
        return pltpu.make_async_remote_copy(
            src_ref=src,
            dst_ref=dst,
            send_sem=send,
            recv_sem=recv,
            device_id=(to_sp, to_dp),
            device_id_type=MESH,
        )

    def arrived(ref, sem):
        pltpu.make_async_copy(ref, ref, sem).wait()

    mine = pl.ds(half * m, half)
    here = pl.ds(pl.multiple_of(m * tokens, tokens), tokens)
    local = [
        pltpu.make_async_copy(ig_hbm.at[mine], igr.at[sp], loc_sem.at[0]),
        pltpu.make_async_copy(fg_hbm.at[mine], fgr.at[sp], loc_sem.at[1]),
        pltpu.make_async_copy(k_hbm.at[mine], xk.at[:, :, here, :], loc_sem.at[2]),
        pltpu.make_async_copy(v_hbm.at[mine], xv.at[:, :, here, :], loc_sem.at[3]),
        pltpu.make_async_copy(q_hbm.at[mine], xq.at[:, :, here, :], loc_sem.at[4]),
        pltpu.make_async_copy(mem_hbm, mem_ref, loc_sem.at[5]),
        pltpu.make_async_copy(norm_hbm, norm_raw, loc_sem.at[6]),
        pltpu.make_async_copy(level_hbm, level_ref, loc_sem.at[7]),
        pltpu.make_async_copy(gain_hbm, gain_ref, loc_sem.at[8]),
        pltpu.make_async_copy(w_hbm, weight.at[dp], loc_sem.at[9]),
    ]
    for copy in local:
        copy.start()

    barrier = pltpu.get_barrier_semaphore()
    for d in range(1, n_sp):
        pl.semaphore_signal(barrier, inc=1, device_id=((sp + d) % n_sp, dp), device_id_type=MESH)
    pl.semaphore_signal(barrier, inc=1, device_id=(sp, twin), device_id_type=MESH)
    for j in range(1, chips):
        pl.semaphore_signal(
            barrier, inc=1, device_id=(sp, ((y + j) % chips) * 2 + core), device_id_type=MESH
        )
    local[5].wait()
    cast[...] = mem_ref[...].astype(bf16)
    local[6].wait()
    norm_ref[...] = jnp.zeros((seqs, heads, width), f32)
    norm_ref[:, :, 0:channels] = norm_raw[...]
    norm_ref[...] = pltpu.roll(
        norm_ref[...].reshape(seqs * heads, width), sp * channels, 1
    ).reshape(seqs, heads, width)
    pl.semaphore_wait(barrier, n_sp - 1 + 1 + chips - 1)

    def gate_copy(d):
        to = (sp + d) % n_sp
        part = pl.ds(half * (to % 2), half)
        return [
            remote(ig_hbm.at[part], igr.at[sp], gate_send.at[0], gate_recv.at[0], to, dp),
            remote(fg_hbm.at[part], fgr.at[sp], gate_send.at[1], gate_recv.at[1], to, dp),
        ]

    def x_copy(kind, c):
        src, dst = ((k_hbm, xk), (v_hbm, xv), (q_hbm, xq))[kind]
        s, h = c // per_seq, (c % per_seq) * PER
        return remote(
            src.at[half * (1 - m) + s, pl.ds(h, PER)],
            dst.at[s, pl.ds(h, PER), here, :],
            x_send.at[kind],
            x_recv.at[kind // 2, c],
            mate,
            dp,
        )

    def own_copy():
        return remote(w_hbm, weight.at[dp], own_send.at[0], own_recv.at[0], sp, twin)

    def piece(r):
        return pl.ds(pl.multiple_of(r * rows, rows), rows)

    direct = PIECES - SKIP - SIDE

    def direct_piece(k):
        side = 2 * SKIP + (1 - m) * SIDE + k - SKIP
        return jnp.where(
            k < SKIP, even * SKIP + k, jnp.where(k < SKIP + SIDE, side, k + SKIP + SIDE)
        )

    def wy_copy(j, k):
        r = piece(direct_piece(k))
        return remote(
            w_hbm.at[r],
            weight.at[dp, r],
            wy_send.at[j],
            wy_recv.at[j, k],
            sp,
            ((y + j) % chips) * 2 + core,
        )

    def wz_copy(j, k, down=True):
        shard = ((y - j + chips) % chips) * 2 + core
        r = piece(direct_piece(k))
        to = lax.rem(sp + n_sp - 2, n_sp) if down else lax.rem(sp + 2, n_sp)
        return remote(
            weight.at[shard, r],
            weight.at[shard, r],
            (wz_send if down else wu_send).at[j],
            wz_recv.at[j],
            to,
            dp,
        )

    def wz_each(j, k, do):
        @pl.when(g > 0)
        def _():
            do(wz_copy(j, k))

        @pl.when(g == n_groups - 2)
        def _():
            do(wz_copy(j, k, down=False))

    def wx_copy(j, k):
        shard = ((y - j + chips) % chips) * 2 + core
        r = piece(direct_piece(k))
        return remote(
            weight.at[shard, r],
            weight.at[shard, r],
            wx_send.at[j],
            wx_recv.at[j],
            mate,
            dp,
        )

    def wd_copy(j, r):
        shard = ((y - j + chips) % chips) * 2 + core
        return remote(
            weight.at[shard, piece(r)],
            weight.at[shard, piece(r)],
            wd_send.at[j],
            wd_recv.at[j],
            sp,
            twin,
        )

    def mem_part(e):
        return e // 2, pl.ds((e % 2) * (heads // 2), heads // 2)

    def mem_cross(e):
        s, h = mem_part(e)
        return remote(
            cast.at[half * (1 - m) + s, h],
            mem_in.at[sp, s, h],
            mem_send.at[0],
            cross_recv.at[e],
            mate,
            dp,
        )

    def mem_cross_arrived(e):
        s, h = mem_part(e)
        return remote(
            cast.at[half * (1 - m) + s, h],
            mem_in.at[mate, s, h],
            mem_send.at[0],
            cross_recv.at[e],
            mate,
            dp,
        )

    def mem_own(e):
        s, h = mem_part(e)
        return remote(
            cast.at[half * m + s, h],
            mem_in.at[sp, s, h],
            mem_send.at[1],
            mem_recv.at[e],
            m,
            dp,
        )

    def mem_mate(e):
        s, h = mem_part(e)
        return remote(
            mem_in.at[mate, s, h],
            mem_in.at[mate, s, h],
            mem_send.at[2],
            mem_recv.at[e],
            m,
            dp,
        )

    def norm_copy(member):
        return remote(
            norm_ref.at[pl.ds(half * member, half)],
            norm_in.at[sp],
            norm_send.at[member],
            norm_recv.at[0],
            member,
            dp,
        )

    for k in range(2):
        for j in range(1, chips):
            wy_copy(j, k).start()
    for e in range(2 * half):
        mem_cross(e).start()
    for d in range(1, n_sp):
        for copy in gate_copy(d):
            copy.start()

    @pl.when(g > 0)
    def _():
        mem_own(0).start()

    for member in range(2):

        @pl.when(sp != member)
        def _():
            norm_copy(member).start()

    @pl.loop(0, chunks)
    def _(c):
        x_copy(0, c).start()
        x_copy(1, c).start()

    @pl.loop(2, direct)
    def _(k):
        for j in range(1, chips):
            wy_copy(j, k).start()

    @pl.loop(0, chunks)
    def _(c):
        x_copy(2, c).start()

    own_copy().start()

    @pl.when(g == 0)
    def _():
        mem_in[sp] = cast[mine]
        norm_in[sp] = norm_ref[mine]

    @pl.when(g > 0)
    def _():
        for e in range(2 * half):
            if e > 0:
                mem_own(e).start()
            mem_cross_arrived(e).wait_recv()
            mem_mate(e).start()

    local[0].wait()
    local[1].wait()
    arrived(igr.at[pl.ds(0, n_sp - 1)], gate_recv.at[0])
    arrived(fgr.at[pl.ds(0, n_sp - 1)], gate_recv.at[1])

    lane = lax.broadcasted_iota(jnp.int32, (n_groups * items, span), 1)

    def whole(ref):
        return jnp.concatenate(
            [
                jnp.concatenate(
                    [
                        ref[2 * i].astype(f32).reshape(items, tokens),
                        ref[2 * i + 1].astype(f32).reshape(items, tokens),
                    ],
                    axis=1,
                )
                for i in range(n_groups)
            ],
            axis=0,
        )

    gate_in = whole(igr)
    pre = whole(fgr)
    total = jnp.minimum(pre, 0.0) - jnp.log1p(jnp.exp(-jnp.abs(pre)))
    step = 1
    while step < span:
        total = total + jnp.where(lane >= step, pltpu.roll(total, step, 1), 0.0)
        step *= 2
    base = jnp.zeros((items, 1), f32)
    parts = []
    for i in range(n_groups):
        part = total[i * items : (i + 1) * items]
        parts.append(gate_in[i * items : (i + 1) * items] - (part + base))
        base = base + part[:, span - 1 : span]
    offset = jnp.concatenate(parts, axis=0)
    peak = offset
    step = 1
    while step < span:
        peak = jnp.maximum(peak, jnp.where(lane >= step, pltpu.roll(peak, step, 1), FILL))
        step *= 2
    local[7].wait()
    local[8].wait()
    eye = lax.broadcasted_iota(jnp.int32, (heads, heads), 0) == lax.broadcasted_iota(
        jnp.int32, (heads, heads), 1
    )
    level = jnp.concatenate(
        [
            jnp.sum(
                jnp.where(eye, level_ref[pl.ds(half * m + i, 1), :], 0.0), axis=1, keepdims=True
            )
            for i in range(half)
        ],
        axis=0,
    )
    level = jnp.broadcast_to(level, (items, span))
    for i in range(n_groups):
        part = peak[i * items : (i + 1) * items]
        starts[i] = level
        offs[i] = offset[i * items : (i + 1) * items]
        peaks[i] = jnp.maximum(part, level)
        level = jnp.maximum(level, jnp.broadcast_to(part[:, span - 1 : span], part.shape))
    starts[n_groups] = level
    first, last = starts[g], starts[g + 1]
    mine_off = offs[g]
    off_g[...] = mine_off
    wrow[...] = jnp.exp(mine_off - last)
    arow[...] = jnp.exp(first - last)
    srow[...] = first
    for copy in local[2:5]:
        copy.wait()

    tail_row = lax.broadcasted_iota(jnp.int32, (TAIL, width), 0)

    def grow(c):
        s, h = c // per_seq, (c % per_seq) * PER
        arrived(xk.at[s, pl.ds(h, PER)], x_recv.at[0, c])
        for p in range(PER):
            key, value = xk[s, h + p], xv[s, h + p]
            w = wrow[pl.ds(c * PER + p, 1), :]
            scaled = (jnp.transpose(key.astype(f32)) * w).astype(bf16)
            grown[c, p, :width] = jnp.dot(scaled, value, preferred_element_type=f32)
            high = w.astype(bf16).astype(f32)
            both = jnp.where(tail_row == 0, high, jnp.where(tail_row == 1, w - high, 0.0))
            norm = jnp.dot(both.astype(bf16), key, preferred_element_type=f32)
            grown[c, p, width:] = jnp.where(tail_row == 0, norm[0:1] + norm[1:2], 0.0)

    def st_copy(c, p):
        return remote(
            st_out.at[c, p],
            st_in.at[c, p],
            st_send.at[0],
            st_recv.at[c, p],
            lax.rem(sp + 2, n_sp),
            dp,
        )

    def seed(c):
        per_part = chunks // (2 * half)

        @pl.when(c % per_part == 0)
        def _():
            e = c // per_part
            mem_cross_arrived(e).wait_recv()
            s, h = e // 2, pl.ds((e % 2) * (heads // 2), heads // 2)
            arrived(mem_in.at[pl.ds(2, n_sp - 2), s, h], mem_recv.at[e])

        @pl.when(c == 0)
        def _():
            arrived(norm_in.at[pl.ds(0, n_sp - 1)], norm_recv.at[0])
            norm = norm_in[0].reshape(items, width)
            for d in range(1, n_sp):
                norm = norm + norm_in[d].reshape(items, width)
            norm_out[...] = norm

        s, h = c // per_seq, (c % per_seq) * PER
        for p in range(PER):
            if channels % 16 == 0:
                st_in[c, p, :width] = mem_in[:, s, h + p].reshape(width, width)
            else:
                for d in range(n_sp):
                    whole_ref[d * channels : (d + 1) * channels] = mem_in[d, s, h + p].astype(f32)
                st_in[c, p, :width] = whole_ref[...].astype(bf16)
            norm = norm_out[pl.ds(c * PER + p, 1), :]
            st_in[c, p, width:] = jnp.where(tail_row == 0, norm, 0.0).astype(bf16)

    def chain(c):
        @pl.when(g == 0)
        def _():
            seed(c)

        for p in range(PER):

            @pl.when(g > 0)
            def _():
                st_copy(c, p).wait_recv()

            @pl.when(g < n_groups - 1)
            def _():
                a = arow[pl.ds(c * PER + p, 1), :]
                st_out[c, p] = (st_in[c, p].astype(f32) * a + grown[c, p]).astype(bf16)
                st_copy(c, p).start()

    def back_copy(c):
        s, h = c // per_seq, (c % per_seq) * PER
        lanes = pl.ds(pl.multiple_of(h * width, PER * width), PER * width)
        return remote(
            back.at[s, :, lanes],
            act.at[half * m + s, :, lanes],
            back_send.at[0],
            back_recv.at[s],
            mate,
            dp,
        )

    t_row = lax.broadcasted_iota(jnp.int32, (span, span), 0)
    s_col = lax.broadcasted_iota(jnp.int32, (span, span), 1)
    causal = s_col <= t_row
    ones = jnp.ones((span, width), bf16)

    def emit(c):
        x_copy(2, c).wait_recv()
        s, h = c // per_seq, (c % per_seq) * PER
        for p in range(PER):
            i = c * PER + p
            query, key, value = xq[s, h + p], xk[s, h + p], xv[s, h + p]
            memory = st_in[c, p, :width]
            norm = jnp.broadcast_to(
                st_in[c, p, width:].astype(f32)[0:1], (width, width)
            ).astype(bf16)
            raw = lax.dot_general(
                query,
                jnp.concatenate([key, norm], axis=0),
                (((1,), (1,)), ((), ())),
                preferred_element_type=f32,
            )
            column = pcol[i]
            gap = jnp.where(causal, off_g[pl.ds(i, 1), :] - column, FILL)
            scores = (raw[:, :span] * factor * jnp.exp(gap)).astype(bf16)
            weigh = jnp.exp(srow[pl.ds(i, 1), :] - column) * factor
            both = jnp.dot(
                scores, jnp.concatenate([value, ones], axis=1), preferred_element_type=f32
            )
            num = both[:, :width] + weigh * jnp.dot(query, memory, preferred_element_type=f32)
            den = both[:, width:] + weigh * raw[:, span:]
            hidden = (num / jnp.maximum(jnp.abs(den), 1.0)).astype(bf16)
            normed = (hidden.astype(f32) * gain_ref[pl.ds(h + p, 1), :]).astype(bf16)
            top, low = normed[:tokens], normed[tokens:]
            lanes = pl.ds(pl.multiple_of((h + p) * width, width), width)
            act[half * m + s, :, lanes] = jnp.where(m == 0, top, low)
            back[s, :, lanes] = jnp.where(m == 0, low, top)
        back_copy(c).start()

    columns_each = weight.shape[2]
    tile = min(512, columns_each)
    tiles = columns_each // tile

    def project(s, first, last):
        left = jnp.concatenate([act[s], act[half + s]], axis=0)

        @pl.loop(first, last)
        def _(n):
            j, b = n // tiles, n % tiles
            shard = ((y + j // 2) % chips) * 2 + (core + j) % 2
            at = pl.ds(pl.multiple_of(b * tile, tile), tile)
            product = jnp.dot(left, weight[shard, :, at], preferred_element_type=f32).astype(bf16)
            to = pl.ds(pl.multiple_of(shard * columns_each + b * tile, tile), tile)
            out_ref[s, :, to] = product[:tokens]
            out_ref[half + s, :, to] = product[tokens:]

    def returned(s):
        arrived(act.at[s], back_recv.at[s])

    own_step = -(-2 * tiles // OWN_SLOTS)
    out_slot = jnp.maximum(chunks, HOP * g)
    slots = max(
        chunks + max(chunks, HOP * (n_groups - 1)),
        WHEN[-1] + 1,
        LATE[-1] + 1,
        WHEN_SKIP + 1,
        WHEN_SIDE + 1,
        WHEN_OWN + OWN_SLOTS,
    )

    def pass_on(j, k):
        wy_copy(j, k).wait_recv()
        wd_copy(j, direct_piece(k)).start()

    @pl.loop(0, slots)
    def _(t):
        @pl.when(t < chunks)
        def _():
            grow(t)

        for k in range(direct):

            @pl.when(t == jnp.where(g == 0, LATE[k], WHEN[k]))
            def _():
                for j in range(1, chips):
                    pass_on(j, k)
                    if k < SKIP:
                        wz_each(j, k, lambda copy: copy.start())
                    elif k < SKIP + SIDE:
                        wx_copy(j, k).start()

        @pl.when(t == WHEN_SKIP)
        def _():
            for j in range(1, chips):
                arrived(weight.at[0, pl.ds(0, SKIP * rows), :], wz_recv.at[j])
                for k in range(SKIP):
                    wd_copy(j, (1 - even) * SKIP + k).start()

        @pl.when(t == jnp.where(g == 0, LATE[-1], WHEN_SIDE))
        def _():
            for j in range(1, chips):
                arrived(weight.at[0, pl.ds(0, SIDE * rows), :], wx_recv.at[j])
                for k in range(SIDE):
                    wd_copy(j, 2 * SKIP + m * SIDE + k).start()

        c = t - HOP * g

        @pl.when((c >= 0) & (c < chunks))
        def _():
            chain(c)

        @pl.when(t == 1)
        def _():
            columns = jnp.transpose(peaks[g])
            for i in range(items):
                pcol[i] = jnp.broadcast_to(columns[:, i : i + 1], (span, span))

        o = t - out_slot

        @pl.when((o >= 0) & (o < chunks))
        def _():
            emit(o)

        @pl.when(t == WHEN_OWN)
        def _():
            returned(0)
            local[9].wait()
            own_copy().wait()

        at_slot = t - WHEN_OWN

        @pl.when((at_slot >= 0) & (at_slot < OWN_SLOTS))
        def _():
            project(0, at_slot * own_step, jnp.minimum((at_slot + 1) * own_step, 2 * tiles))

    def left_all(ref, sem):
        pltpu.make_async_copy(ref, ref, sem).wait()

    def sent_early():
        left_all(igr.at[pl.ds(0, n_sp - 1)], gate_send.at[0])
        left_all(fgr.at[pl.ds(0, n_sp - 1)], gate_send.at[1])
        for kind, ref in enumerate((xk, xv, xq)):
            left_all(ref.at[:, :, pl.ds(0, tokens), :], x_send.at[kind])
        left_all(mem_in.at[0], mem_send.at[0])

        @pl.when(g > 0)
        def _():
            left_all(mem_in.at[0], mem_send.at[1])
            left_all(mem_in.at[0], mem_send.at[2])

        for member in range(2):

            @pl.when(sp != member)
            def _():
                norm_copy(member).wait_send()

    def sent_late():
        left_all(back, back_send.at[0])

        @pl.when(g < n_groups - 1)
        def _():
            left_all(st_out, st_send.at[0])

        for j in range(1, chips):
            left_all(weight.at[0, pl.ds(0, direct * rows), :], wy_send.at[j])
            left_all(weight.at[0], wd_send.at[j])

            @pl.when(g > 0)
            def _():
                left_all(weight.at[0, pl.ds(0, SKIP * rows), :], wz_send.at[j])

            @pl.when(g == n_groups - 2)
            def _():
                left_all(weight.at[0, pl.ds(0, SKIP * rows), :], wu_send.at[j])

            left_all(weight.at[0, pl.ds(0, SIDE * rows), :], wx_send.at[j])

    for j in range(1, chips):
        arrived(weight.at[0], wd_recv.at[j])
    project(0, 2 * tiles, n_dp * tiles)
    sent_early()
    for s in range(1, half):
        returned(s)
        project(s, 0, n_dp * tiles)
    sent_late()


def on_device(
    queries,
    keys,
    values,
    input_gate,
    forget_gate,
    start_memory,
    start_norm,
    start_level,
    head_gain,
    out_weight,
):
    seqs, heads, tokens, width = queries.shape
    n_sp, n_dp = lax.axis_size("sp"), lax.axis_size("dp")
    channels = start_memory.shape[2]
    mix, columns = out_weight.shape
    half = seqs // 2
    items = half * heads
    span = 2 * tokens
    groups = n_sp // 2
    chips = n_dp // 2
    chunks = items // PER
    direct = PIECES - SKIP - SIDE
    f32, bf16 = jnp.float32, jnp.bfloat16
    sizes = (n_sp, n_dp, seqs, heads, tokens, width, channels)
    operands = [
        pltpu.with_memory_space_constraint(array, pltpu.HBM)
        for array in (
            queries,
            keys,
            values,
            input_gate,
            forget_gate,
            out_weight,
            start_memory,
            start_norm,
            start_level,
            head_gain,
        )
    ]
    hbm_spec = pl.BlockSpec(memory_space=pltpu.HBM)
    vmem = pl.BlockSpec(memory_space=pltpu.VMEM)
    dma = pltpu.SemaphoreType.DMA
    return pl.pallas_call(
        lambda *refs: layer_kernel(sizes, *refs),
        out_shape=jax.ShapeDtypeStruct((seqs, tokens, n_dp * columns), bf16),
        in_specs=[hbm_spec] * len(operands),
        out_specs=vmem,
        scratch_shapes=[
            pltpu.VMEM((seqs, heads, channels, width), f32),
            pltpu.VMEM((seqs, heads, channels), f32),
            pltpu.VMEM((seqs, heads), f32),
            pltpu.VMEM((heads, width), f32),
            pltpu.VMEM((seqs, heads, width), f32),
            pltpu.VMEM((half, heads, span, width), bf16),
            pltpu.VMEM((half, heads, span, width), bf16),
            pltpu.VMEM((half, heads, span, width), bf16),
            pltpu.VMEM((n_sp, half, heads, tokens), bf16),
            pltpu.VMEM((n_sp, half, heads, tokens), bf16),
            pltpu.VMEM((seqs, heads, channels, width), bf16),
            pltpu.VMEM((n_sp, half, heads, channels, width), bf16),
            pltpu.VMEM((n_sp, half, heads, width), f32),
            pltpu.VMEM((items, width), f32),
            pltpu.VMEM((width, width), f32),
            pltpu.VMEM((groups, items, span), f32),
            pltpu.VMEM((groups, items, span), f32),
            pltpu.VMEM((groups + 1, items, span), f32),
            pltpu.VMEM((items, span), f32),
            pltpu.VMEM((items, span), f32),
            pltpu.VMEM((items, span), f32),
            pltpu.VMEM((items, span), f32),
            pltpu.VMEM((items, span, span), f32),
            pltpu.VMEM((chunks, PER, width + TAIL, width), f32),
            pltpu.VMEM((chunks, PER, width + TAIL, width), bf16),
            pltpu.VMEM((chunks, PER, width + TAIL, width), bf16),
            pltpu.VMEM((seqs, tokens, heads * width), bf16),
            pltpu.VMEM((half, tokens, heads * width), bf16),
            pltpu.VMEM((n_dp, mix, columns), bf16),
            dma((10,)),
            dma((2,)),
            dma((2,)),
            dma((3,)),
            dma((2, chunks)),
            dma((3,)),
            dma((2 * half,)),
            dma((2 * half,)),
            dma((2,)),
            dma((1,)),
            dma((1,)),
            dma((chunks, PER)),
            dma((1,)),
            dma((half,)),
            dma((chips,)),
            dma((chips, direct)),
            dma((chips,)),
            dma((chips,)),
            dma((chips,)),
            dma((chips,)),
            dma((chips,)),
            dma((chips,)),
            dma((chips,)),
            dma((1,)),
            dma((1,)),
        ],
        compiler_params=pltpu.CompilerParams(
            collective_id=0, has_side_effects=True, vmem_limit_bytes=40 * 1024 * 1024
        ),
        name="layer",
    )(*operands)


def solution(mesh):
    in_specs = (
        P("dp", None, "sp", None),
        P("dp", None, "sp", None),
        P("dp", None, "sp", None),
        P("dp", None, "sp"),
        P("dp", None, "sp"),
        P("dp", None, "sp", None),
        P("dp", None, "sp"),
        P("dp", None),
        P(),
        P(None, "dp"),
    )
    out_specs = P("dp", "sp", None)
    return jax.shard_map(
        on_device, mesh=mesh, in_specs=in_specs, out_specs=out_specs, check_vma=False
    )
```

```python
import jax
import jax.numpy as jnp
from jax import lax
from jax.experimental import pallas as pl
from jax.experimental.pallas import tpu as pltpu
from jax.sharding import PartitionSpec as P

MESH = pl.DeviceIdType.MESH
FILL = -1e30
PER = 2
HOP = 3
PIECES = 16
SKIP = 4
SIDE = 2
WHEN = (0, 2, 4, 6, 8, 10)
LATE = (8, 8, 8, 8, 9, 12)
REST = (12, 14, 15, 15)
WHEN_SKIP = 13
WHEN_SIDE = 15
OWN_SLOTS = 3
WHEN_OWN = 14
TAIL = 8


def layer_kernel(
    sizes,
    q_hbm,
    k_hbm,
    v_hbm,
    ig_hbm,
    fg_hbm,
    w_hbm,
    mem_hbm,
    norm_hbm,
    level_hbm,
    gain_hbm,
    out_ref,
    mem_ref,
    norm_raw,
    level_ref,
    gain_ref,
    norm_ref,
    xq,
    xk,
    xv,
    igr,
    fgr,
    cast,
    mem_in,
    norm_in,
    norm_out,
    whole_ref,
    offs,
    peaks,
    starts,
    off_g,
    wrow,
    into,
    upon,
    arow,
    srow,
    pcol,
    grown,
    st_in,
    st_out,
    act,
    back,
    weight,
    loc_sem,
    gate_send,
    gate_recv,
    x_send,
    x_recv,
    mem_send,
    cross_recv,
    mem_recv,
    down_send,
    norm_recv,
    st_send,
    st_recv,
    back_send,
    back_recv,
    wy_send,
    wy_recv,
    wz_send,
    wu_send,
    wz_recv,
    wx_send,
    wx_recv,
    wf_send,
    wf_recv,
    wd_send,
    wd_recv,
    own_send,
    own_recv,
):
    n_sp, n_dp, seqs, heads, tokens, width, channels = sizes
    n_groups = n_sp // 2
    chips = n_dp // 2
    half = seqs // 2
    items = half * heads
    span = 2 * tokens
    chunks = items // PER
    per_seq = heads // PER
    rows = w_hbm.shape[0] // PIECES
    factor = width ** (-0.5)
    f32, bf16 = jnp.float32, jnp.bfloat16

    sp, dp = lax.axis_index("sp"), lax.axis_index("dp")
    g, m = sp // 2, sp % 2
    y, core = dp // 2, dp % 2
    mate = g * 2 + (1 - m)
    twin = y * 2 + (1 - core)
    even = 1 - g % 2

    def remote(src, dst, send, recv, to_sp, to_dp):
        return pltpu.make_async_remote_copy(
            src_ref=src,
            dst_ref=dst,
            send_sem=send,
            recv_sem=recv,
            device_id=(to_sp, to_dp),
            device_id_type=MESH,
        )

    def arrived(ref, sem):
        pltpu.make_async_copy(ref, ref, sem).wait()

    mine = pl.ds(half * m, half)
    here = pl.ds(pl.multiple_of(m * tokens, tokens), tokens)
    local = [
        pltpu.make_async_copy(ig_hbm.at[mine], igr.at[sp], loc_sem.at[0]),
        pltpu.make_async_copy(fg_hbm.at[mine], fgr.at[sp], loc_sem.at[1]),
        pltpu.make_async_copy(k_hbm.at[mine], xk.at[:, :, here, :], loc_sem.at[2]),
        pltpu.make_async_copy(v_hbm.at[mine], xv.at[:, :, here, :], loc_sem.at[3]),
        pltpu.make_async_copy(q_hbm.at[mine], xq.at[:, :, here, :], loc_sem.at[4]),
        pltpu.make_async_copy(mem_hbm, mem_ref, loc_sem.at[5]),
        pltpu.make_async_copy(norm_hbm, norm_raw, loc_sem.at[6]),
        pltpu.make_async_copy(level_hbm, level_ref, loc_sem.at[7]),
        pltpu.make_async_copy(gain_hbm, gain_ref, loc_sem.at[8]),
        pltpu.make_async_copy(w_hbm, weight.at[dp], loc_sem.at[9]),
    ]
    for copy in local:
        copy.start()

    barrier = pltpu.get_barrier_semaphore()
    for d in range(1, n_sp):
        pl.semaphore_signal(barrier, inc=1, device_id=((sp + d) % n_sp, dp), device_id_type=MESH)
    pl.semaphore_signal(barrier, inc=1, device_id=(sp, twin), device_id_type=MESH)
    for j in range(1, chips):
        pl.semaphore_signal(
            barrier, inc=1, device_id=(sp, ((y + j) % chips) * 2 + core), device_id_type=MESH
        )
    local[5].wait()
    cast[...] = mem_ref[...].astype(bf16)
    local[6].wait()
    norm_ref[...] = jnp.zeros((seqs, heads, width), f32)
    norm_ref[:, :, 0:channels] = norm_raw[...]
    norm_ref[...] = pltpu.roll(
        norm_ref[...].reshape(seqs * heads, width), sp * channels, 1
    ).reshape(seqs, heads, width)
    pl.semaphore_wait(barrier, n_sp - 1 + 1 + chips - 1)

    def gate_copy(d):
        to = (sp + d) % n_sp
        part = pl.ds(half * (to % 2), half)
        return [
            remote(ig_hbm.at[part], igr.at[sp], gate_send.at[0], gate_recv.at[0], to, dp),
            remote(fg_hbm.at[part], fgr.at[sp], gate_send.at[1], gate_recv.at[1], to, dp),
        ]

    def x_copy(kind, c):
        src, dst = ((k_hbm, xk), (v_hbm, xv), (q_hbm, xq))[kind]
        s, h = c // per_seq, (c % per_seq) * PER
        return remote(
            src.at[half * (1 - m) + s, pl.ds(h, PER)],
            dst.at[s, pl.ds(h, PER), here, :],
            x_send.at[kind],
            x_recv.at[kind // 2, c],
            mate,
            dp,
        )

    def own_copy():
        return remote(w_hbm, weight.at[dp], own_send.at[0], own_recv.at[0], sp, twin)

    def piece(r):
        return pl.ds(pl.multiple_of(r * rows, rows), rows)

    direct = PIECES - SKIP - SIDE

    def direct_piece(k):
        side = 2 * SKIP + (1 - m) * SIDE + k - SKIP
        both = 2 * SKIP + m * SIDE + k - SKIP - SIDE
        rest = jnp.where((g == 0) & (k < SKIP + 2 * SIDE), both, k + SKIP + SIDE)
        return jnp.where(k < SKIP, even * SKIP + k, jnp.where(k < SKIP + SIDE, side, rest))

    def wy_copy(j, k):
        r = piece(direct_piece(k))
        return remote(
            w_hbm.at[r],
            weight.at[dp, r],
            wy_send.at[j],
            wy_recv.at[j, k],
            sp,
            ((y + j) % chips) * 2 + core,
        )

    def wz_copy(j, k, down=True):
        shard = ((y - j + chips) % chips) * 2 + core
        r = piece(direct_piece(k))
        to = lax.rem(sp + n_sp - 2, n_sp) if down else lax.rem(sp + 2, n_sp)
        return remote(
            weight.at[shard, r],
            weight.at[shard, r],
            (wz_send if down else wu_send).at[j],
            wz_recv.at[j],
            to,
            dp,
        )

    def wz_each(j, k, do):
        @pl.when(g > 0)
        def _():
            do(wz_copy(j, k))

        @pl.when(g == n_groups - 2)
        def _():
            do(wz_copy(j, k, down=False))

    def wf_copy(j, k):
        shard = ((y - j + chips) % chips) * 2 + core
        r = piece(k + SKIP + SIDE)
        return remote(
            weight.at[shard, r],
            weight.at[shard, r],
            wf_send.at[j],
            wf_recv.at[j],
            lax.rem(sp + n_sp - 2, n_sp),
            dp,
        )

    def wx_copy(j, k):
        shard = ((y - j + chips) % chips) * 2 + core
        r = piece(direct_piece(k))
        return remote(
            weight.at[shard, r],
            weight.at[shard, r],
            wx_send.at[j],
            wx_recv.at[j],
            mate,
            dp,
        )

    def wd_copy(j, r):
        shard = ((y - j + chips) % chips) * 2 + core
        return remote(
            weight.at[shard, piece(r)],
            weight.at[shard, piece(r)],
            wd_send.at[j],
            wd_recv.at[j],
            sp,
            twin,
        )

    def mem_cross(at):
        return remote(
            cast.at[pl.ds(half * (1 - m), half)],
            mem_in.at[at],
            mem_send.at[0],
            cross_recv.at[0],
            mate,
            dp,
        )

    def norm_cross(at):
        return remote(
            norm_ref.at[pl.ds(half * (1 - m), half)],
            norm_in.at[at],
            mem_send.at[1],
            cross_recv.at[1],
            mate,
            dp,
        )

    def mem_down(d):
        to = lax.rem(sp + n_sp - 2 * d, n_sp)
        return [
            remote(cast.at[mine], mem_in.at[sp], down_send.at[0, d], mem_recv.at[g], to, dp),
            remote(norm_ref.at[mine], norm_in.at[sp], down_send.at[1, d], norm_recv.at[g], to, dp),
        ]

    def mem_relay(d):
        to = lax.rem(sp + n_sp - 2 * d, n_sp)
        return [
            remote(
                mem_in.at[mate], mem_in.at[mate], down_send.at[2, d], mem_recv.at[g], to, dp
            ),
            remote(
                norm_in.at[mate], norm_in.at[mate], down_send.at[3, d], norm_recv.at[g], to, dp
            ),
        ]

    for k in range(2):
        for j in range(1, chips):
            wy_copy(j, k).start()
    for d in range(1, n_sp):
        for copy in gate_copy(d):
            copy.start()
    mem_cross(sp).start()
    norm_cross(sp).start()

    @pl.loop(0, chunks)
    def _(c):
        x_copy(0, c).start()
        x_copy(1, c).start()

    @pl.loop(2, direct)
    def _(k):
        for j in range(1, chips):
            wy_copy(j, k).start()

    @pl.loop(0, chunks)
    def _(c):
        x_copy(2, c).start()

    own_copy().start()
    for d in range(1, n_groups):

        @pl.when(g >= d)
        def _():
            for copy in mem_down(d):
                copy.start()

    @pl.when(g == 0)
    def _():
        st_in[...] = jnp.zeros(st_in.shape, bf16)

    mem_in[sp] = cast[mine]
    norm_in[sp] = norm_ref[mine]
    for i in range(n_groups):

        @pl.when(i < g)
        def _():
            mem_in[2 * i : 2 * i + 2] = jnp.zeros((2, half, heads, channels, width), bf16)
            norm_in[2 * i : 2 * i + 2] = jnp.zeros((2, half, heads, width), f32)

    mem_cross(mate).wait_recv()
    norm_cross(mate).wait_recv()
    for d in range(1, n_groups):

        @pl.when(g >= d)
        def _():
            for copy in mem_relay(d):
                copy.start()

    local[0].wait()
    local[1].wait()
    arrived(igr.at[pl.ds(0, n_sp - 1)], gate_recv.at[0])
    arrived(fgr.at[pl.ds(0, n_sp - 1)], gate_recv.at[1])

    lane = lax.broadcasted_iota(jnp.int32, (n_groups * items, span), 1)

    def whole(ref):
        return jnp.concatenate(
            [
                jnp.concatenate(
                    [
                        ref[2 * i].astype(f32).reshape(items, tokens),
                        ref[2 * i + 1].astype(f32).reshape(items, tokens),
                    ],
                    axis=1,
                )
                for i in range(n_groups)
            ],
            axis=0,
        )

    gate_in = whole(igr)
    pre = whole(fgr)
    total = jnp.minimum(pre, 0.0) - jnp.log1p(jnp.exp(-jnp.abs(pre)))
    step = 1
    while step < span:
        total = total + jnp.where(lane >= step, pltpu.roll(total, step, 1), 0.0)
        step *= 2
    base = jnp.zeros((items, 1), f32)
    parts = []
    for i in range(n_groups):
        part = total[i * items : (i + 1) * items]
        parts.append(gate_in[i * items : (i + 1) * items] - (part + base))
        base = base + part[:, span - 1 : span]
    offset = jnp.concatenate(parts, axis=0)
    peak = offset
    step = 1
    while step < span:
        peak = jnp.maximum(peak, jnp.where(lane >= step, pltpu.roll(peak, step, 1), FILL))
        step *= 2
    local[7].wait()
    local[8].wait()
    eye = lax.broadcasted_iota(jnp.int32, (heads, heads), 0) == lax.broadcasted_iota(
        jnp.int32, (heads, heads), 1
    )
    level = jnp.concatenate(
        [
            jnp.sum(
                jnp.where(eye, level_ref[pl.ds(half * m + i, 1), :], 0.0), axis=1, keepdims=True
            )
            for i in range(half)
        ],
        axis=0,
    )
    level = jnp.broadcast_to(level, (items, span))
    for i in range(n_groups):
        part = peak[i * items : (i + 1) * items]
        starts[i] = level
        offs[i] = offset[i * items : (i + 1) * items]
        peaks[i] = jnp.maximum(part, level)
        level = jnp.maximum(level, jnp.broadcast_to(part[:, span - 1 : span], part.shape))
    starts[n_groups] = level
    first, last = starts[g], starts[g + 1]
    into[...] = jnp.exp(starts[0] - last)
    upon[...] = jnp.exp(starts[0] - first)
    mine_off = offs[g]
    off_g[...] = mine_off
    wrow[...] = jnp.exp(mine_off - last)
    arow[...] = jnp.exp(first - last)
    srow[...] = first
    for copy in local[2:5]:
        copy.wait()

    w_row = lax.broadcasted_iota(jnp.int32, (16, width), 0)
    tail_row = lax.broadcasted_iota(jnp.int32, (TAIL, width), 0)

    def grow(c):
        s, h = c // per_seq, (c % per_seq) * PER
        arrived(xk.at[s, pl.ds(h, PER)], x_recv.at[0, c])
        for p in range(PER):
            key, value = xk[s, h + p], xv[s, h + p]
            w = wrow[pl.ds(c * PER + p, 1), :]
            scaled = (jnp.transpose(key.astype(f32)) * w).astype(bf16)
            grown[c, p, :width] = jnp.dot(scaled, value, preferred_element_type=f32)
            start = into[pl.ds(c * PER + p, 1), :]
            for i in range(2):
                whole_ref[i * channels : (i + 1) * channels] = mem_in[2 * g + i, s, h + p].astype(
                    f32
                )
            rows_here = pl.ds(pl.multiple_of(g * 2 * channels, 2 * channels), 2 * channels)
            grown[c, p, rows_here] += whole_ref[0 : 2 * channels] * start
            high = w.astype(bf16).astype(f32)
            both = jnp.where(w_row == 0, high, jnp.where(w_row == 1, w - high, 0.0))
            norm = jnp.dot(both.astype(bf16), key, preferred_element_type=f32)
            norm = norm[0:1] + norm[1:2]
            for i in range(2):
                norm = norm + norm_in[2 * g + i, s, pl.ds(h + p, 1), :] * start
            grown[c, p, width:] = jnp.where(tail_row == 0, norm, 0.0)

    def st_copy(c, p):
        return remote(
            st_out.at[c, p],
            st_in.at[c, p],
            st_send.at[0],
            st_recv.at[c, p],
            lax.rem(sp + 2, n_sp),
            dp,
        )

    def initial(s, h):
        if channels % 16 == 0:
            return mem_in[:, s, h].reshape(width, width).astype(f32)
        for d in range(n_sp):
            whole_ref[d * channels : (d + 1) * channels] = mem_in[d, s, h].astype(f32)
        return whole_ref[...]

    def initial_arrived():
        for i in range(1, n_groups):

            @pl.when(i > g)
            def _():
                arrived(mem_in.at[pl.ds(2 * i, 2)], mem_recv.at[i])
                arrived(norm_in.at[pl.ds(2 * i, 2)], norm_recv.at[i])

        norm = norm_in[0].reshape(items, width)
        for d in range(1, n_sp):
            norm = norm + norm_in[d].reshape(items, width)
        norm_out[...] = norm

    def chain(c):
        for p in range(PER):

            @pl.when(g > 0)
            def _():
                st_copy(c, p).wait_recv()

            @pl.when(g < n_groups - 1)
            def _():
                a = arow[pl.ds(c * PER + p, 1), :]
                st_out[c, p] = (st_in[c, p].astype(f32) * a + grown[c, p]).astype(bf16)
                st_copy(c, p).start()

    def back_copy(c):
        s, h = c // per_seq, (c % per_seq) * PER
        lanes = pl.ds(pl.multiple_of(h * width, PER * width), PER * width)
        return remote(
            back.at[s, :, lanes],
            act.at[half * m + s, :, lanes],
            back_send.at[0],
            back_recv.at[s],
            mate,
            dp,
        )

    t_row = lax.broadcasted_iota(jnp.int32, (span, span), 0)
    s_col = lax.broadcasted_iota(jnp.int32, (span, span), 1)
    causal = s_col <= t_row
    ones = jnp.ones((span, width), bf16)

    def emit(c):
        x_copy(2, c).wait_recv()
        s, h = c // per_seq, (c % per_seq) * PER
        for p in range(PER):
            i = c * PER + p
            query, key, value = xq[s, h + p], xk[s, h + p], xv[s, h + p]
            start = upon[pl.ds(i, 1), :]
            memory = (
                st_in[c, p, :width].astype(f32) + initial(s, h + p) * start
            ).astype(bf16)
            norm = st_in[c, p, width:].astype(f32)[0:1] + norm_out[pl.ds(i, 1), :] * start
            norm = jnp.broadcast_to(norm, (width, width)).astype(bf16)
            raw = lax.dot_general(
                query,
                jnp.concatenate([key, norm], axis=0),
                (((1,), (1,)), ((), ())),
                preferred_element_type=f32,
            )
            column = pcol[i]
            gap = jnp.where(causal, off_g[pl.ds(i, 1), :] - column, FILL)
            scores = (raw[:, :span] * factor * jnp.exp(gap)).astype(bf16)
            weigh = jnp.exp(srow[pl.ds(i, 1), :] - column) * factor
            both = jnp.dot(
                scores, jnp.concatenate([value, ones], axis=1), preferred_element_type=f32
            )
            num = both[:, :width] + weigh * jnp.dot(query, memory, preferred_element_type=f32)
            den = both[:, width:] + weigh * raw[:, span:]
            hidden = (num / jnp.maximum(jnp.abs(den), 1.0)).astype(bf16)
            normed = (hidden.astype(f32) * gain_ref[pl.ds(h + p, 1), :]).astype(bf16)
            top, low = normed[:tokens], normed[tokens:]
            lanes = pl.ds(pl.multiple_of((h + p) * width, width), width)
            act[half * m + s, :, lanes] = jnp.where(m == 0, top, low)
            back[s, :, lanes] = jnp.where(m == 0, low, top)
        back_copy(c).start()

    columns_each = weight.shape[2]
    tile = min(512, columns_each)
    tiles = columns_each // tile

    def project(which, first, last):
        picked = [base + s for s in which for base in (0, half)]
        left = jnp.concatenate([act[i] for i in picked], axis=0)

        @pl.loop(first, last)
        def _(n):
            j, b = n // tiles, n % tiles
            shard = ((y + j // 2) % chips) * 2 + (core + j) % 2
            at = pl.ds(pl.multiple_of(b * tile, tile), tile)
            product = jnp.dot(left, weight[shard, :, at], preferred_element_type=f32).astype(bf16)
            to = pl.ds(pl.multiple_of(shard * columns_each + b * tile, tile), tile)
            for n_row, i in enumerate(picked):
                out_ref[i, :, to] = product[n_row * tokens : (n_row + 1) * tokens]

    def own_here():
        local[9].wait()
        own_copy().wait()

    def returned(s):
        arrived(act.at[s], back_recv.at[s])

    own_step = -(-2 * tiles // OWN_SLOTS)
    out_slot = jnp.maximum(chunks, HOP * g)
    slots = max(
        chunks + max(chunks, HOP * (n_groups - 1)),
        REST[-1] + 1,
        WHEN_SKIP + 1,
        WHEN_SIDE + 1,
        WHEN_OWN + OWN_SLOTS,
    )

    def pass_on(j, k):
        wy_copy(j, k).wait_recv()
        wd_copy(j, direct_piece(k)).start()

    def pass_rest(k):
        for j in range(1, chips):
            pass_on(j, k)
            if k < SKIP + 2 * SIDE:

                @pl.when(g == 1)
                def _():
                    wf_copy(j, k).start()

    def pass_first():
        for j in range(1, chips):
            arrived(weight.at[0, pl.ds(0, SIDE * rows), :], wf_recv.at[j])
            for k in range(SIDE):
                wd_copy(j, 2 * SKIP + 2 * SIDE + k).start()

    def pass_skip():
        for j in range(1, chips):
            arrived(weight.at[0, pl.ds(0, SKIP * rows), :], wz_recv.at[j])
            for k in range(SKIP):
                wd_copy(j, (1 - even) * SKIP + k).start()

    def pass_side():
        for j in range(1, chips):
            arrived(weight.at[0, pl.ds(0, SIDE * rows), :], wx_recv.at[j])
            for k in range(SIDE):
                wd_copy(j, 2 * SKIP + m * SIDE + k).start()

    @pl.loop(0, slots)
    def _(t):
        @pl.when(t < chunks)
        def _():
            grow(t)

        for k in range(SKIP + SIDE):

            @pl.when(t == jnp.where(g == 0, LATE[k], WHEN[k]))
            def _():
                for j in range(1, chips):
                    pass_on(j, k)
                    if k < SKIP:
                        wz_each(j, k, lambda copy: copy.start())
                    else:

                        @pl.when(g > 0)
                        def _():
                            wx_copy(j, k).start()

        for k in range(SKIP + SIDE, direct):

            @pl.when((g == n_groups - 1) & (t == REST[k - SKIP - SIDE]))
            def _():
                pass_rest(k)

        @pl.when((g == n_groups - 1) & (t == WHEN_SKIP))
        def _():
            pass_skip()

        @pl.when((g == n_groups - 1) & (t == WHEN_SIDE))
        def _():
            pass_side()

        c = t - HOP * g

        @pl.when((c >= 0) & (c < chunks))
        def _():
            chain(c)

        @pl.when(t == 1)
        def _():
            columns = jnp.transpose(peaks[g])
            for i in range(items):
                pcol[i] = jnp.broadcast_to(columns[:, i : i + 1], (span, span))

        @pl.when(t == out_slot)
        def _():
            initial_arrived()

        o = t - out_slot

        @pl.when((o >= 0) & (o < chunks))
        def _():
            emit(o)

        @pl.when((g == n_groups - 1) & (t == WHEN_OWN))
        def _():
            returned(0)
            own_here()

        at_slot = t - WHEN_OWN

        @pl.when((g == n_groups - 1) & (at_slot >= 0) & (at_slot < OWN_SLOTS))
        def _():
            project([0], at_slot * own_step, jnp.minimum((at_slot + 1) * own_step, 2 * tiles))

    def left_all(ref, sem):
        pltpu.make_async_copy(ref, ref, sem).wait()

    def sent_early():
        left_all(igr.at[pl.ds(0, n_sp - 1)], gate_send.at[0])
        left_all(fgr.at[pl.ds(0, n_sp - 1)], gate_send.at[1])
        for kind, ref in enumerate((xk, xv, xq)):
            left_all(ref.at[:, :, pl.ds(0, tokens), :], x_send.at[kind])
        mem_cross(sp).wait_send()
        norm_cross(sp).wait_send()
        for d in range(1, n_groups):

            @pl.when(g >= d)
            def _():
                for copy in mem_down(d) + mem_relay(d):
                    copy.wait_send()

    def sent_late():
        left_all(back, back_send.at[0])

        @pl.when(g < n_groups - 1)
        def _():
            left_all(st_out, st_send.at[0])

        for j in range(1, chips):
            left_all(weight.at[0, pl.ds(0, direct * rows), :], wy_send.at[j])
            left_all(weight.at[0], wd_send.at[j])

            @pl.when(g > 0)
            def _():
                left_all(weight.at[0, pl.ds(0, SKIP * rows), :], wz_send.at[j])

            @pl.when(g == n_groups - 2)
            def _():
                left_all(weight.at[0, pl.ds(0, SKIP * rows), :], wu_send.at[j])

            @pl.when(g > 0)
            def _():
                left_all(weight.at[0, pl.ds(0, SIDE * rows), :], wx_send.at[j])

            @pl.when(g == 1)
            def _():
                left_all(weight.at[0, pl.ds(0, SIDE * rows), :], wf_send.at[j])

    def twin_arrived():
        for j in range(1, chips):
            arrived(weight.at[0], wd_recv.at[j])

    every = list(range(half))
    near, far = 2 * tiles, n_dp * tiles

    @pl.when(g == n_groups - 1)
    def _():
        twin_arrived()
        project([0], near, far)
        sent_early()
        for s in every[1:]:
            returned(s)
        project(every[1:], 0, far)

    @pl.when(g < n_groups - 1)
    def _():
        first = SKIP + SIDE
        pass_rest(first)
        pass_rest(first + 1)
        pass_skip()
        pass_rest(first + 2)

        def ready():
            own_here()
            for s in every:
                returned(s)

        @pl.when(g == 0)
        def _():
            ready()
            project(every, 0, near - 1)

        @pl.when(g > 0)
        def _():
            pass_side()

        for k in range(first + 3, direct):
            pass_rest(k)

        @pl.when(g == 0)
        def _():
            pass_first()

        @pl.when(g > 0)
        def _():
            ready()

        project(every, jnp.where(g == 0, near - 1, 0), near)
        sent_early()
        twin_arrived()
        project(every, near, far)

    sent_late()


def on_device(
    queries,
    keys,
    values,
    input_gate,
    forget_gate,
    start_memory,
    start_norm,
    start_level,
    head_gain,
    out_weight,
):
    seqs, heads, tokens, width = queries.shape
    n_sp, n_dp = lax.axis_size("sp"), lax.axis_size("dp")
    channels = start_memory.shape[2]
    mix, columns = out_weight.shape
    half = seqs // 2
    items = half * heads
    span = 2 * tokens
    groups = n_sp // 2
    chips = n_dp // 2
    chunks = items // PER
    direct = PIECES - SKIP - SIDE
    f32, bf16 = jnp.float32, jnp.bfloat16
    sizes = (n_sp, n_dp, seqs, heads, tokens, width, channels)
    operands = [
        pltpu.with_memory_space_constraint(array, pltpu.HBM)
        for array in (
            queries,
            keys,
            values,
            input_gate,
            forget_gate,
            out_weight,
            start_memory,
            start_norm,
            start_level,
            head_gain,
        )
    ]
    hbm_spec = pl.BlockSpec(memory_space=pltpu.HBM)
    vmem = pl.BlockSpec(memory_space=pltpu.VMEM)
    dma = pltpu.SemaphoreType.DMA
    return pl.pallas_call(
        lambda *refs: layer_kernel(sizes, *refs),
        out_shape=jax.ShapeDtypeStruct((seqs, tokens, n_dp * columns), bf16),
        in_specs=[hbm_spec] * len(operands),
        out_specs=vmem,
        scratch_shapes=[
            pltpu.VMEM((seqs, heads, channels, width), f32),
            pltpu.VMEM((seqs, heads, channels), f32),
            pltpu.VMEM((seqs, heads), f32),
            pltpu.VMEM((heads, width), f32),
            pltpu.VMEM((seqs, heads, width), f32),
            pltpu.VMEM((half, heads, span, width), bf16),
            pltpu.VMEM((half, heads, span, width), bf16),
            pltpu.VMEM((half, heads, span, width), bf16),
            pltpu.VMEM((n_sp, half, heads, tokens), bf16),
            pltpu.VMEM((n_sp, half, heads, tokens), bf16),
            pltpu.VMEM((seqs, heads, channels, width), bf16),
            pltpu.VMEM((n_sp, half, heads, channels, width), bf16),
            pltpu.VMEM((n_sp, half, heads, width), f32),
            pltpu.VMEM((items, width), f32),
            pltpu.VMEM((width, width), f32),
            pltpu.VMEM((groups, items, span), f32),
            pltpu.VMEM((groups, items, span), f32),
            pltpu.VMEM((groups + 1, items, span), f32),
            pltpu.VMEM((items, span), f32),
            pltpu.VMEM((items, span), f32),
            pltpu.VMEM((items, span), f32),
            pltpu.VMEM((items, span), f32),
            pltpu.VMEM((items, span), f32),
            pltpu.VMEM((items, span), f32),
            pltpu.VMEM((items, span, span), f32),
            pltpu.VMEM((chunks, PER, width + TAIL, width), f32),
            pltpu.VMEM((chunks, PER, width + TAIL, width), bf16),
            pltpu.VMEM((chunks, PER, width + TAIL, width), bf16),
            pltpu.VMEM((seqs, tokens, heads * width), bf16),
            pltpu.VMEM((half, tokens, heads * width), bf16),
            pltpu.VMEM((n_dp, mix, columns), bf16),
            dma((10,)),
            dma((2,)),
            dma((2,)),
            dma((3,)),
            dma((2, chunks)),
            dma((2,)),
            dma((2,)),
            dma((groups,)),
            dma((4, groups)),
            dma((groups,)),
            dma((1,)),
            dma((chunks, PER)),
            dma((1,)),
            dma((half,)),
            dma((chips,)),
            dma((chips, direct)),
            dma((chips,)),
            dma((chips,)),
            dma((chips,)),
            dma((chips,)),
            dma((chips,)),
            dma((chips,)),
            dma((chips,)),
            dma((chips,)),
            dma((chips,)),
            dma((1,)),
            dma((1,)),
        ],
        compiler_params=pltpu.CompilerParams(
            collective_id=0, has_side_effects=True, vmem_limit_bytes=40 * 1024 * 1024
        ),
        name="layer",
    )(*operands)


def solution(mesh):
    in_specs = (
        P("dp", None, "sp", None),
        P("dp", None, "sp", None),
        P("dp", None, "sp", None),
        P("dp", None, "sp"),
        P("dp", None, "sp"),
        P("dp", None, "sp", None),
        P("dp", None, "sp"),
        P("dp", None),
        P(),
        P(None, "dp"),
    )
    out_specs = P("dp", "sp", None)
    return jax.shard_map(
        on_device, mesh=mesh, in_specs=in_specs, out_specs=out_specs, check_vma=False
    )
```

```python
import jax
import jax.numpy as jnp
from jax import lax
from jax.experimental import pallas as pl
from jax.experimental.pallas import tpu as pltpu
from jax.sharding import PartitionSpec as P

MESH = pl.DeviceIdType.MESH
FILL = -1e30
PER = 2
HOP = 3
PIECES = 16
SKIP = 4
UP = 3
SIDE = 2
WHEN = (0, 2, 4, 6, 8, 10)
LATE = (8, 8, 8, 8, 9, 12)
REST = (12, 14)
WHEN_SKIP = 13
TAIL = 8


def layer_kernel(
    sizes,
    q_hbm,
    k_hbm,
    v_hbm,
    ig_hbm,
    fg_hbm,
    w_hbm,
    mem_hbm,
    norm_hbm,
    level_hbm,
    gain_hbm,
    out_ref,
    mem_ref,
    norm_raw,
    level_ref,
    gain_ref,
    norm_ref,
    xq,
    xk,
    xv,
    igr,
    fgr,
    cast,
    mem_in,
    norm_in,
    norm_out,
    whole_ref,
    offs,
    peaks,
    starts,
    off_g,
    wrow,
    into,
    upon,
    arow,
    srow,
    pcol,
    grown,
    st_in,
    st_out,
    act,
    back,
    weight,
    loc_sem,
    gate_send,
    gate_recv,
    x_send,
    x_recv,
    mem_send,
    cross_recv,
    mem_recv,
    down_send,
    norm_recv,
    st_send,
    st_recv,
    back_send,
    back_recv,
    wy_send,
    wy_recv,
    wz_send,
    wu_send,
    wz_recv,
    wx_send,
    wx_recv,
    wf_send,
    wf_recv,
    wd_send,
    wd_recv,
    own_send,
    own_recv,
):
    n_sp, n_dp, seqs, heads, tokens, width, channels = sizes
    n_groups = n_sp // 2
    chips = n_dp // 2
    half = seqs // 2
    items = half * heads
    span = 2 * tokens
    chunks = items // PER
    per_seq = heads // PER
    rows = w_hbm.shape[0] // PIECES
    factor = width ** (-0.5)
    f32, bf16 = jnp.float32, jnp.bfloat16

    sp, dp = lax.axis_index("sp"), lax.axis_index("dp")
    g, m = sp // 2, sp % 2
    y, core = dp // 2, dp % 2
    mate = g * 2 + (1 - m)
    twin = y * 2 + (1 - core)
    even = 1 - g % 2

    def remote(src, dst, send, recv, to_sp, to_dp):
        return pltpu.make_async_remote_copy(
            src_ref=src,
            dst_ref=dst,
            send_sem=send,
            recv_sem=recv,
            device_id=(to_sp, to_dp),
            device_id_type=MESH,
        )

    def arrived(ref, sem):
        pltpu.make_async_copy(ref, ref, sem).wait()

    mine = pl.ds(half * m, half)
    here = pl.ds(pl.multiple_of(m * tokens, tokens), tokens)
    local = [
        pltpu.make_async_copy(ig_hbm.at[mine], igr.at[sp], loc_sem.at[0]),
        pltpu.make_async_copy(fg_hbm.at[mine], fgr.at[sp], loc_sem.at[1]),
        pltpu.make_async_copy(k_hbm.at[mine], xk.at[:, :, here, :], loc_sem.at[2]),
        pltpu.make_async_copy(v_hbm.at[mine], xv.at[:, :, here, :], loc_sem.at[3]),
        pltpu.make_async_copy(q_hbm.at[mine], xq.at[:, :, here, :], loc_sem.at[4]),
        pltpu.make_async_copy(mem_hbm, mem_ref, loc_sem.at[5]),
        pltpu.make_async_copy(norm_hbm, norm_raw, loc_sem.at[6]),
        pltpu.make_async_copy(level_hbm, level_ref, loc_sem.at[7]),
        pltpu.make_async_copy(gain_hbm, gain_ref, loc_sem.at[8]),
        pltpu.make_async_copy(w_hbm, weight.at[dp], loc_sem.at[9]),
    ]
    for copy in local:
        copy.start()

    barrier = pltpu.get_barrier_semaphore()
    for d in range(1, n_sp):
        pl.semaphore_signal(barrier, inc=1, device_id=((sp + d) % n_sp, dp), device_id_type=MESH)
    pl.semaphore_signal(barrier, inc=1, device_id=(sp, twin), device_id_type=MESH)
    for j in range(1, chips):
        pl.semaphore_signal(
            barrier, inc=1, device_id=(sp, ((y + j) % chips) * 2 + core), device_id_type=MESH
        )
    local[5].wait()
    cast[...] = mem_ref[...].astype(bf16)
    local[6].wait()
    norm_ref[...] = jnp.zeros((seqs, heads, width), f32)
    norm_ref[:, :, 0:channels] = norm_raw[...]
    norm_ref[...] = pltpu.roll(
        norm_ref[...].reshape(seqs * heads, width), sp * channels, 1
    ).reshape(seqs, heads, width)
    pl.semaphore_wait(barrier, n_sp - 1 + 1 + chips - 1)

    def gate_copy(d):
        to = (sp + d) % n_sp
        part = pl.ds(half * (to % 2), half)
        return [
            remote(ig_hbm.at[part], igr.at[sp], gate_send.at[0], gate_recv.at[0], to, dp),
            remote(fg_hbm.at[part], fgr.at[sp], gate_send.at[1], gate_recv.at[1], to, dp),
        ]

    def x_copy(kind, c):
        src, dst = ((k_hbm, xk), (v_hbm, xv), (q_hbm, xq))[kind]
        s, h = c // per_seq, (c % per_seq) * PER
        return remote(
            src.at[half * (1 - m) + s, pl.ds(h, PER)],
            dst.at[s, pl.ds(h, PER), here, :],
            x_send.at[kind],
            x_recv.at[kind // 2, c],
            mate,
            dp,
        )

    def own_copy():
        return remote(w_hbm, weight.at[dp], own_send.at[0], own_recv.at[0], sp, twin)

    def piece(r):
        return pl.ds(pl.multiple_of(r * rows, rows), rows)

    direct = PIECES - SKIP - SIDE

    def direct_piece(k):
        side = 2 * SKIP + (1 - m) * SIDE + k - SKIP
        both = 2 * SKIP + m * SIDE + k - SKIP - SIDE
        rest = jnp.where((g == 0) & (k < SKIP + 2 * SIDE), both, k + SKIP + SIDE)
        piece_at = jnp.where(k < SKIP, even * SKIP + k, jnp.where(k < SKIP + SIDE, side, rest))
        return jnp.where(k < direct, piece_at, (1 - even) * SKIP + UP + k - direct)

    def wy_copy(j, k):
        r = piece(direct_piece(k))
        return remote(
            w_hbm.at[r],
            weight.at[dp, r],
            wy_send.at[j],
            wy_recv.at[j, k],
            sp,
            ((y + j) % chips) * 2 + core,
        )

    def wz_copy(j, k, down=True):
        shard = ((y - j + chips) % chips) * 2 + core
        r = piece(direct_piece(k))
        to = lax.rem(sp + n_sp - 2, n_sp) if down else lax.rem(sp + 2, n_sp)
        return remote(
            weight.at[shard, r],
            weight.at[shard, r],
            (wz_send if down else wu_send).at[j],
            wz_recv.at[j],
            to,
            dp,
        )

    def wz_each(j, k, do):
        @pl.when(g > 0)
        def _():
            do(wz_copy(j, k))

        if k < UP:

            @pl.when(g == n_groups - 2)
            def _():
                do(wz_copy(j, k, down=False))

    def wf_copy(j, k):
        shard = ((y - j + chips) % chips) * 2 + core
        r = piece(k + SKIP + SIDE)
        return remote(
            weight.at[shard, r],
            weight.at[shard, r],
            wf_send.at[j],
            wf_recv.at[j],
            lax.rem(sp + n_sp - 2, n_sp),
            dp,
        )

    def wx_copy(j, k):
        shard = ((y - j + chips) % chips) * 2 + core
        r = piece(direct_piece(k))
        return remote(
            weight.at[shard, r],
            weight.at[shard, r],
            wx_send.at[j],
            wx_recv.at[j],
            mate,
            dp,
        )

    def wd_copy(j, r):
        shard = ((y - j + chips) % chips) * 2 + core
        return remote(
            weight.at[shard, piece(r)],
            weight.at[shard, piece(r)],
            wd_send.at[j],
            wd_recv.at[j],
            sp,
            twin,
        )

    def mem_cross(at):
        return remote(
            cast.at[pl.ds(half * (1 - m), half)],
            mem_in.at[at],
            mem_send.at[0],
            cross_recv.at[0],
            mate,
            dp,
        )

    def norm_cross(at):
        return remote(
            norm_ref.at[pl.ds(half * (1 - m), half)],
            norm_in.at[at],
            mem_send.at[1],
            cross_recv.at[1],
            mate,
            dp,
        )

    def mem_down(d):
        to = lax.rem(sp + n_sp - 2 * d, n_sp)
        return [
            remote(cast.at[mine], mem_in.at[sp], down_send.at[0, d], mem_recv.at[g], to, dp),
            remote(norm_ref.at[mine], norm_in.at[sp], down_send.at[1, d], norm_recv.at[g], to, dp),
        ]

    def mem_relay(d):
        to = lax.rem(sp + n_sp - 2 * d, n_sp)
        return [
            remote(
                mem_in.at[mate], mem_in.at[mate], down_send.at[2, d], mem_recv.at[g], to, dp
            ),
            remote(
                norm_in.at[mate], norm_in.at[mate], down_send.at[3, d], norm_recv.at[g], to, dp
            ),
        ]

    for k in range(2):
        for j in range(1, chips):
            wy_copy(j, k).start()
    for d in range(1, n_sp):
        for copy in gate_copy(d):
            copy.start()
    mem_cross(sp).start()
    norm_cross(sp).start()

    @pl.loop(0, chunks)
    def _(c):
        x_copy(0, c).start()
        x_copy(1, c).start()

    @pl.loop(2, direct)
    def _(k):
        for j in range(1, chips):
            wy_copy(j, k).start()

    @pl.when(g == n_groups - 1)
    def _():
        for k in range(direct, direct + SKIP - UP):
            for j in range(1, chips):
                wy_copy(j, k).start()

    @pl.loop(0, chunks)
    def _(c):
        x_copy(2, c).start()

    own_copy().start()
    for d in range(1, n_groups):

        @pl.when(g >= d)
        def _():
            for copy in mem_down(d):
                copy.start()

    @pl.when(g == 0)
    def _():
        st_in[...] = jnp.zeros(st_in.shape, bf16)

    mem_in[sp] = cast[mine]
    norm_in[sp] = norm_ref[mine]
    for i in range(n_groups):

        @pl.when(i < g)
        def _():
            mem_in[2 * i : 2 * i + 2] = jnp.zeros((2, half, heads, channels, width), bf16)
            norm_in[2 * i : 2 * i + 2] = jnp.zeros((2, half, heads, width), f32)

    mem_cross(mate).wait_recv()
    norm_cross(mate).wait_recv()
    for d in range(1, n_groups):

        @pl.when(g >= d)
        def _():
            for copy in mem_relay(d):
                copy.start()

    local[0].wait()
    local[1].wait()
    arrived(igr.at[pl.ds(0, n_sp - 1)], gate_recv.at[0])
    arrived(fgr.at[pl.ds(0, n_sp - 1)], gate_recv.at[1])

    lane = lax.broadcasted_iota(jnp.int32, (n_groups * items, span), 1)

    def whole(ref):
        return jnp.concatenate(
            [
                jnp.concatenate(
                    [
                        ref[2 * i].astype(f32).reshape(items, tokens),
                        ref[2 * i + 1].astype(f32).reshape(items, tokens),
                    ],
                    axis=1,
                )
                for i in range(n_groups)
            ],
            axis=0,
        )

    gate_in = whole(igr)
    pre = whole(fgr)
    total = jnp.minimum(pre, 0.0) - jnp.log1p(jnp.exp(-jnp.abs(pre)))
    step = 1
    while step < span:
        total = total + jnp.where(lane >= step, pltpu.roll(total, step, 1), 0.0)
        step *= 2
    base = jnp.zeros((items, 1), f32)
    parts = []
    for i in range(n_groups):
        part = total[i * items : (i + 1) * items]
        parts.append(gate_in[i * items : (i + 1) * items] - (part + base))
        base = base + part[:, span - 1 : span]
    offset = jnp.concatenate(parts, axis=0)
    peak = offset
    step = 1
    while step < span:
        peak = jnp.maximum(peak, jnp.where(lane >= step, pltpu.roll(peak, step, 1), FILL))
        step *= 2
    local[7].wait()
    local[8].wait()
    eye = lax.broadcasted_iota(jnp.int32, (heads, heads), 0) == lax.broadcasted_iota(
        jnp.int32, (heads, heads), 1
    )
    level = jnp.concatenate(
        [
            jnp.sum(
                jnp.where(eye, level_ref[pl.ds(half * m + i, 1), :], 0.0), axis=1, keepdims=True
            )
            for i in range(half)
        ],
        axis=0,
    )
    level = jnp.broadcast_to(level, (items, span))
    for i in range(n_groups):
        part = peak[i * items : (i + 1) * items]
        starts[i] = level
        offs[i] = offset[i * items : (i + 1) * items]
        peaks[i] = jnp.maximum(part, level)
        level = jnp.maximum(level, jnp.broadcast_to(part[:, span - 1 : span], part.shape))
    starts[n_groups] = level
    first, last = starts[g], starts[g + 1]
    into[...] = jnp.exp(starts[0] - last)
    upon[...] = jnp.exp(starts[0] - first)
    mine_off = offs[g]
    off_g[...] = mine_off
    wrow[...] = jnp.exp(mine_off - last)
    arow[...] = jnp.exp(first - last)
    srow[...] = first
    for copy in local[2:5]:
        copy.wait()

    w_row = lax.broadcasted_iota(jnp.int32, (16, width), 0)
    tail_row = lax.broadcasted_iota(jnp.int32, (TAIL, width), 0)

    def grow(c):
        s, h = c // per_seq, (c % per_seq) * PER
        arrived(xk.at[s, pl.ds(h, PER)], x_recv.at[0, c])
        for p in range(PER):
            key, value = xk[s, h + p], xv[s, h + p]
            w = wrow[pl.ds(c * PER + p, 1), :]
            scaled = (jnp.transpose(key.astype(f32)) * w).astype(bf16)
            grown[c, p, :width] = jnp.dot(scaled, value, preferred_element_type=f32)
            start = into[pl.ds(c * PER + p, 1), :]
            for i in range(2):
                whole_ref[i * channels : (i + 1) * channels] = mem_in[2 * g + i, s, h + p].astype(
                    f32
                )
            rows_here = pl.ds(pl.multiple_of(g * 2 * channels, 2 * channels), 2 * channels)
            grown[c, p, rows_here] += whole_ref[0 : 2 * channels] * start
            high = w.astype(bf16).astype(f32)
            both = jnp.where(w_row == 0, high, jnp.where(w_row == 1, w - high, 0.0))
            norm = jnp.dot(both.astype(bf16), key, preferred_element_type=f32)
            norm = norm[0:1] + norm[1:2]
            for i in range(2):
                norm = norm + norm_in[2 * g + i, s, pl.ds(h + p, 1), :] * start
            grown[c, p, width:] = jnp.where(tail_row == 0, norm, 0.0)

    def st_copy(c, p):
        return remote(
            st_out.at[c, p],
            st_in.at[c, p],
            st_send.at[0],
            st_recv.at[c, p],
            lax.rem(sp + 2, n_sp),
            dp,
        )

    def initial(s, h):
        if channels % 16 == 0:
            return mem_in[:, s, h].reshape(width, width).astype(f32)
        for d in range(n_sp):
            whole_ref[d * channels : (d + 1) * channels] = mem_in[d, s, h].astype(f32)
        return whole_ref[...]

    def initial_arrived():
        for i in range(1, n_groups):

            @pl.when(i > g)
            def _():
                arrived(mem_in.at[pl.ds(2 * i, 2)], mem_recv.at[i])
                arrived(norm_in.at[pl.ds(2 * i, 2)], norm_recv.at[i])

        norm = norm_in[0].reshape(items, width)
        for d in range(1, n_sp):
            norm = norm + norm_in[d].reshape(items, width)
        norm_out[...] = norm

    def chain(c):
        for p in range(PER):

            @pl.when(g > 0)
            def _():
                st_copy(c, p).wait_recv()

            @pl.when(g < n_groups - 1)
            def _():
                a = arow[pl.ds(c * PER + p, 1), :]
                st_out[c, p] = (st_in[c, p].astype(f32) * a + grown[c, p]).astype(bf16)
                st_copy(c, p).start()

    def back_copy(c):
        s, h = c // per_seq, (c % per_seq) * PER
        lanes = pl.ds(pl.multiple_of(h * width, PER * width), PER * width)
        return remote(
            back.at[s, :, lanes],
            act.at[half * m + s, :, lanes],
            back_send.at[0],
            back_recv.at[s],
            mate,
            dp,
        )

    t_row = lax.broadcasted_iota(jnp.int32, (span, span), 0)
    s_col = lax.broadcasted_iota(jnp.int32, (span, span), 1)
    causal = s_col <= t_row
    ones = jnp.ones((span, width), bf16)

    def emit(c):
        x_copy(2, c).wait_recv()
        s, h = c // per_seq, (c % per_seq) * PER
        for p in range(PER):
            i = c * PER + p
            query, key, value = xq[s, h + p], xk[s, h + p], xv[s, h + p]
            start = upon[pl.ds(i, 1), :]
            memory = (
                st_in[c, p, :width].astype(f32) + initial(s, h + p) * start
            ).astype(bf16)
            norm = st_in[c, p, width:].astype(f32)[0:1] + norm_out[pl.ds(i, 1), :] * start
            norm = jnp.broadcast_to(norm, (width, width)).astype(bf16)
            raw = lax.dot_general(
                query,
                jnp.concatenate([key, norm], axis=0),
                (((1,), (1,)), ((), ())),
                preferred_element_type=f32,
            )
            column = pcol[i]
            gap = jnp.where(causal, off_g[pl.ds(i, 1), :] - column, FILL)
            scores = (raw[:, :span] * factor * jnp.exp(gap)).astype(bf16)
            weigh = jnp.exp(srow[pl.ds(i, 1), :] - column) * factor
            both = jnp.dot(
                scores, jnp.concatenate([value, ones], axis=1), preferred_element_type=f32
            )
            num = both[:, :width] + weigh * jnp.dot(query, memory, preferred_element_type=f32)
            den = both[:, width:] + weigh * raw[:, span:]
            hidden = (num / jnp.maximum(jnp.abs(den), 1.0)).astype(bf16)
            normed = (hidden.astype(f32) * gain_ref[pl.ds(h + p, 1), :]).astype(bf16)
            top, low = normed[:tokens], normed[tokens:]
            lanes = pl.ds(pl.multiple_of((h + p) * width, width), width)
            act[half * m + s, :, lanes] = jnp.where(m == 0, top, low)
            back[s, :, lanes] = jnp.where(m == 0, low, top)
        back_copy(c).start()

    columns_each = weight.shape[2]
    tile = min(1024, columns_each)
    tiles = columns_each // tile

    def project(which, first, last):
        picked = [base + s for s in which for base in (0, half)]
        left = jnp.concatenate([act[i] for i in picked], axis=0)

        for n in range(first, last):
            j, b = n // tiles, n % tiles
            shard = ((y + j // 2) % chips) * 2 + (core + j) % 2
            at = pl.ds(b * tile, tile)
            product = jnp.dot(left, weight[shard, :, at], preferred_element_type=f32).astype(bf16)
            to = pl.ds(pl.multiple_of(shard * columns_each + b * tile, tile), tile)
            for n_row, i in enumerate(picked):
                out_ref[i, :, to] = product[n_row * tokens : (n_row + 1) * tokens]

    def own_here():
        local[9].wait()
        own_copy().wait()

    def returned(s):
        arrived(act.at[s], back_recv.at[s])
    out_slot = jnp.maximum(chunks, HOP * g)
    slots = max(
        chunks + max(chunks, HOP * (n_groups - 1)),
        REST[-1] + 1,
        WHEN_SKIP + 1,
    )

    def pass_on(j, k):
        wy_copy(j, k).wait_recv()
        wd_copy(j, direct_piece(k)).start()

    def pass_rest(k):
        for j in range(1, chips):
            pass_on(j, k)
            if k < SKIP + 2 * SIDE:

                @pl.when(g == 1)
                def _():
                    wf_copy(j, k).start()

    def pass_first():
        for j in range(1, chips):
            arrived(weight.at[0, pl.ds(0, SIDE * rows), :], wf_recv.at[j])
            for k in range(SIDE):
                wd_copy(j, 2 * SKIP + 2 * SIDE + k).start()

    def pass_skip(count):
        for j in range(1, chips):
            arrived(weight.at[0, pl.ds(0, count * rows), :], wz_recv.at[j])
            for k in range(count):
                wd_copy(j, (1 - even) * SKIP + k).start()

    def pass_side():
        for j in range(1, chips):
            arrived(weight.at[0, pl.ds(0, SIDE * rows), :], wx_recv.at[j])
            for k in range(SIDE):
                wd_copy(j, 2 * SKIP + m * SIDE + k).start()

    @pl.loop(0, slots)
    def _(t):
        @pl.when(t < chunks)
        def _():
            grow(t)

        for k in range(SKIP + SIDE):

            @pl.when(t == jnp.where(g == 0, LATE[k], WHEN[k]))
            def _():
                for j in range(1, chips):
                    pass_on(j, k)
                    if k < SKIP:
                        wz_each(j, k, lambda copy: copy.start())
                    else:

                        @pl.when(g > 0)
                        def _():
                            wx_copy(j, k).start()

        for k in range(SKIP + SIDE, SKIP + SIDE + len(REST)):

            @pl.when((g == n_groups - 1) & (t == REST[k - SKIP - SIDE]))
            def _():
                pass_rest(k)

        @pl.when((g == n_groups - 1) & (t == WHEN_SKIP))
        def _():
            pass_skip(UP)

        c = t - HOP * g

        @pl.when((c >= 0) & (c < chunks))
        def _():
            chain(c)

        @pl.when(t == 1)
        def _():
            columns = jnp.transpose(peaks[g])
            for i in range(items):
                pcol[i] = jnp.broadcast_to(columns[:, i : i + 1], (span, span))

        @pl.when(t == out_slot)
        def _():
            initial_arrived()

        o = t - out_slot

        @pl.when((o >= 0) & (o < chunks))
        def _():
            emit(o)

    def left_all(ref, sem):
        pltpu.make_async_copy(ref, ref, sem).wait()

    def sent_early():
        left_all(igr.at[pl.ds(0, n_sp - 1)], gate_send.at[0])
        left_all(fgr.at[pl.ds(0, n_sp - 1)], gate_send.at[1])
        for kind, ref in enumerate((xk, xv, xq)):
            left_all(ref.at[:, :, pl.ds(0, tokens), :], x_send.at[kind])
        mem_cross(sp).wait_send()
        norm_cross(sp).wait_send()
        for d in range(1, n_groups):

            @pl.when(g >= d)
            def _():
                for copy in mem_down(d) + mem_relay(d):
                    copy.wait_send()

        left_all(back, back_send.at[0])

        @pl.when(g < n_groups - 1)
        def _():
            left_all(st_out, st_send.at[0])

        for j in range(1, chips):

            @pl.when(g > 0)
            def _():
                left_all(weight.at[0, pl.ds(0, SKIP * rows), :], wz_send.at[j])
                left_all(weight.at[0, pl.ds(0, SIDE * rows), :], wx_send.at[j])

            @pl.when(g == n_groups - 2)
            def _():
                left_all(weight.at[0, pl.ds(0, UP * rows), :], wu_send.at[j])

            @pl.when(g == 1)
            def _():
                left_all(weight.at[0, pl.ds(0, SIDE * rows), :], wf_send.at[j])

    def sent_late():
        for j in range(1, chips):
            left_all(weight.at[0, pl.ds(0, direct * rows), :], wy_send.at[j])
            left_all(weight.at[0], wd_send.at[j])

            @pl.when(g == n_groups - 1)
            def _():
                left_all(weight.at[0, pl.ds(0, (SKIP - UP) * rows), :], wy_send.at[j])

    def twin_arrived():
        for j in range(1, chips):
            arrived(weight.at[0], wd_recv.at[j])

    every = list(range(half))
    near, far = 2 * tiles, n_dp * tiles

    first = SKIP + SIDE

    @pl.when(g < n_groups - 1)
    def _():
        for k in range(first, first + len(REST)):
            pass_rest(k)
        pass_skip(SKIP)

    for k in range(first + len(REST), direct - 1):
        pass_rest(k)

    @pl.when(g > 0)
    def _():
        pass_side()
        pass_rest(direct - 1)

    sent_early()
    own_here()
    for s in every:
        returned(s)

    project(every, 0, max(1, near // 2))

    @pl.when(g == 0)
    def _():
        pass_rest(direct - 1)
        pass_first()

    @pl.when(g == n_groups - 1)
    def _():
        for k in range(direct, direct + SKIP - UP):
            for j in range(1, chips):
                pass_on(j, k)

    project(every, max(1, near // 2), near)
    twin_arrived()
    project(every, near, far)
    sent_late()


def on_device(
    queries,
    keys,
    values,
    input_gate,
    forget_gate,
    start_memory,
    start_norm,
    start_level,
    head_gain,
    out_weight,
):
    seqs, heads, tokens, width = queries.shape
    n_sp, n_dp = lax.axis_size("sp"), lax.axis_size("dp")
    channels = start_memory.shape[2]
    mix, columns = out_weight.shape
    half = seqs // 2
    items = half * heads
    span = 2 * tokens
    groups = n_sp // 2
    chips = n_dp // 2
    chunks = items // PER
    direct = PIECES - SKIP - SIDE
    f32, bf16 = jnp.float32, jnp.bfloat16
    sizes = (n_sp, n_dp, seqs, heads, tokens, width, channels)
    operands = [
        pltpu.with_memory_space_constraint(array, pltpu.HBM)
        for array in (
            queries,
            keys,
            values,
            input_gate,
            forget_gate,
            out_weight,
            start_memory,
            start_norm,
            start_level,
            head_gain,
        )
    ]
    hbm_spec = pl.BlockSpec(memory_space=pltpu.HBM)
    vmem = pl.BlockSpec(memory_space=pltpu.VMEM)
    dma = pltpu.SemaphoreType.DMA
    return pl.pallas_call(
        lambda *refs: layer_kernel(sizes, *refs),
        out_shape=jax.ShapeDtypeStruct((seqs, tokens, n_dp * columns), bf16),
        in_specs=[hbm_spec] * len(operands),
        out_specs=vmem,
        scratch_shapes=[
            pltpu.VMEM((seqs, heads, channels, width), f32),
            pltpu.VMEM((seqs, heads, channels), f32),
            pltpu.VMEM((seqs, heads), f32),
            pltpu.VMEM((heads, width), f32),
            pltpu.VMEM((seqs, heads, width), f32),
            pltpu.VMEM((half, heads, span, width), bf16),
            pltpu.VMEM((half, heads, span, width), bf16),
            pltpu.VMEM((half, heads, span, width), bf16),
            pltpu.VMEM((n_sp, half, heads, tokens), bf16),
            pltpu.VMEM((n_sp, half, heads, tokens), bf16),
            pltpu.VMEM((seqs, heads, channels, width), bf16),
            pltpu.VMEM((n_sp, half, heads, channels, width), bf16),
            pltpu.VMEM((n_sp, half, heads, width), f32),
            pltpu.VMEM((items, width), f32),
            pltpu.VMEM((width, width), f32),
            pltpu.VMEM((groups, items, span), f32),
            pltpu.VMEM((groups, items, span), f32),
            pltpu.VMEM((groups + 1, items, span), f32),
            pltpu.VMEM((items, span), f32),
            pltpu.VMEM((items, span), f32),
            pltpu.VMEM((items, span), f32),
            pltpu.VMEM((items, span), f32),
            pltpu.VMEM((items, span), f32),
            pltpu.VMEM((items, span), f32),
            pltpu.VMEM((items, span, span), f32),
            pltpu.VMEM((chunks, PER, width + TAIL, width), f32),
            pltpu.VMEM((chunks, PER, width + TAIL, width), bf16),
            pltpu.VMEM((chunks, PER, width + TAIL, width), bf16),
            pltpu.VMEM((seqs, tokens, heads * width), bf16),
            pltpu.VMEM((half, tokens, heads * width), bf16),
            pltpu.VMEM((n_dp, mix, columns), bf16),
            dma((10,)),
            dma((2,)),
            dma((2,)),
            dma((3,)),
            dma((2, chunks)),
            dma((2,)),
            dma((2,)),
            dma((groups,)),
            dma((4, groups)),
            dma((groups,)),
            dma((1,)),
            dma((chunks, PER)),
            dma((1,)),
            dma((half,)),
            dma((chips,)),
            dma((chips, direct + SKIP - UP)),
            dma((chips,)),
            dma((chips,)),
            dma((chips,)),
            dma((chips,)),
            dma((chips,)),
            dma((chips,)),
            dma((chips,)),
            dma((chips,)),
            dma((chips,)),
            dma((1,)),
            dma((1,)),
        ],
        compiler_params=pltpu.CompilerParams(
            collective_id=0, has_side_effects=True, vmem_limit_bytes=40 * 1024 * 1024
        ),
        name="layer",
    )(*operands)


def solution(mesh):
    in_specs = (
        P("dp", None, "sp", None),
        P("dp", None, "sp", None),
        P("dp", None, "sp", None),
        P("dp", None, "sp"),
        P("dp", None, "sp"),
        P("dp", None, "sp", None),
        P("dp", None, "sp"),
        P("dp", None),
        P(),
        P(None, "dp"),
    )
    out_specs = P("dp", "sp", None)
    return jax.shard_map(
        on_device, mesh=mesh, in_specs=in_specs, out_specs=out_specs, check_vma=False
    )
```

```python
import jax
import jax.numpy as jnp
from jax import lax
from jax.experimental import pallas as pl
from jax.experimental.pallas import tpu as pltpu
from jax.sharding import PartitionSpec as P

MESH = pl.DeviceIdType.MESH
FILL = -1e30
PER = 2
HOP = 3
PIECES = 16
SKIP = 4
UP = 3
SIDE = 2
WHEN = (0, 2, 4, 6, 8, 10)
LATE = (8, 8, 8, 8, 9, 12)
REST = (12, 14)
WHEN_SKIP = 13
TAIL = 8


def layer_kernel(
    sizes,
    q_hbm,
    k_hbm,
    v_hbm,
    ig_hbm,
    fg_hbm,
    w_hbm,
    mem_hbm,
    norm_hbm,
    level_hbm,
    gain_hbm,
    out_ref,
    mem_ref,
    norm_raw,
    level_ref,
    gain_ref,
    norm_ref,
    xq,
    xk,
    xv,
    igr,
    fgr,
    cast,
    mem_in,
    norm_in,
    norm_out,
    whole_ref,
    offs,
    peaks,
    starts,
    off_g,
    wrow,
    into,
    upon,
    arow,
    srow,
    pcol,
    grown,
    st_in,
    st_out,
    act,
    back,
    weight,
    loc_sem,
    gate_send,
    gate_recv,
    x_send,
    x_recv,
    mem_send,
    cross_recv,
    mem_recv,
    down_send,
    norm_recv,
    st_send,
    st_recv,
    back_send,
    back_recv,
    wy_send,
    wy_recv,
    wz_send,
    wu_send,
    wz_recv,
    wx_send,
    wx_recv,
    wf_send,
    wf_recv,
    wd_send,
    wd_recv,
    own_send,
    own_recv,
):
    n_sp, n_dp, seqs, heads, tokens, width, channels = sizes
    n_groups = n_sp // 2
    chips = n_dp // 2
    half = seqs // 2
    items = half * heads
    span = 2 * tokens
    chunks = items // PER
    per_seq = heads // PER
    rows = w_hbm.shape[0] // PIECES
    factor = width ** (-0.5)
    f32, bf16 = jnp.float32, jnp.bfloat16

    sp, dp = lax.axis_index("sp"), lax.axis_index("dp")
    g, m = sp // 2, sp % 2
    y, core = dp // 2, dp % 2
    mate = g * 2 + (1 - m)
    twin = y * 2 + (1 - core)
    even = 1 - g % 2

    def remote(src, dst, send, recv, to_sp, to_dp):
        return pltpu.make_async_remote_copy(
            src_ref=src,
            dst_ref=dst,
            send_sem=send,
            recv_sem=recv,
            device_id=(to_sp, to_dp),
            device_id_type=MESH,
        )

    def arrived(ref, sem):
        pltpu.make_async_copy(ref, ref, sem).wait()

    mine = pl.ds(half * m, half)
    here = pl.ds(pl.multiple_of(m * tokens, tokens), tokens)
    local = [
        pltpu.make_async_copy(ig_hbm.at[mine], igr.at[sp], loc_sem.at[0]),
        pltpu.make_async_copy(fg_hbm.at[mine], fgr.at[sp], loc_sem.at[1]),
        pltpu.make_async_copy(k_hbm.at[mine], xk.at[:, :, here, :], loc_sem.at[2]),
        pltpu.make_async_copy(v_hbm.at[mine], xv.at[:, :, here, :], loc_sem.at[3]),
        pltpu.make_async_copy(q_hbm.at[mine], xq.at[:, :, here, :], loc_sem.at[4]),
        pltpu.make_async_copy(mem_hbm, mem_ref, loc_sem.at[5]),
        pltpu.make_async_copy(norm_hbm, norm_raw, loc_sem.at[6]),
        pltpu.make_async_copy(level_hbm, level_ref, loc_sem.at[7]),
        pltpu.make_async_copy(gain_hbm, gain_ref, loc_sem.at[8]),
        pltpu.make_async_copy(w_hbm, weight.at[dp], loc_sem.at[9]),
    ]
    for copy in local:
        copy.start()

    barrier = pltpu.get_barrier_semaphore()
    for d in range(1, n_sp):
        pl.semaphore_signal(barrier, inc=1, device_id=((sp + d) % n_sp, dp), device_id_type=MESH)
    pl.semaphore_signal(barrier, inc=1, device_id=(sp, twin), device_id_type=MESH)
    for j in range(1, chips):
        pl.semaphore_signal(
            barrier, inc=1, device_id=(sp, ((y + j) % chips) * 2 + core), device_id_type=MESH
        )
    local[5].wait()
    cast[...] = mem_ref[...].astype(bf16)
    local[6].wait()
    norm_ref[...] = jnp.zeros((seqs, heads, width), f32)
    norm_ref[:, :, 0:channels] = norm_raw[...]
    norm_ref[...] = pltpu.roll(
        norm_ref[...].reshape(seqs * heads, width), sp * channels, 1
    ).reshape(seqs, heads, width)
    pl.semaphore_wait(barrier, n_sp - 1 + 1 + chips - 1)

    def gate_copy(d):
        to = (sp + d) % n_sp
        part = pl.ds(half * (to % 2), half)
        return [
            remote(ig_hbm.at[part], igr.at[sp], gate_send.at[0], gate_recv.at[0], to, dp),
            remote(fg_hbm.at[part], fgr.at[sp], gate_send.at[1], gate_recv.at[1], to, dp),
        ]

    def x_copy(kind, c):
        src, dst = ((k_hbm, xk), (v_hbm, xv), (q_hbm, xq))[kind]
        s, h = c // per_seq, (c % per_seq) * PER
        return remote(
            src.at[half * (1 - m) + s, pl.ds(h, PER)],
            dst.at[s, pl.ds(h, PER), here, :],
            x_send.at[kind],
            x_recv.at[kind // 2, c],
            mate,
            dp,
        )

    def own_copy():
        return remote(w_hbm, weight.at[dp], own_send.at[0], own_recv.at[0], sp, twin)

    def piece(r):
        return pl.ds(pl.multiple_of(r * rows, rows), rows)

    direct = PIECES - SKIP - SIDE

    def direct_piece(k):
        side = 2 * SKIP + (1 - m) * SIDE + k - SKIP
        both = 2 * SKIP + m * SIDE + k - SKIP - SIDE
        rest = jnp.where((g == 0) & (k < SKIP + 2 * SIDE), both, k + SKIP + SIDE)
        piece_at = jnp.where(k < SKIP, even * SKIP + k, jnp.where(k < SKIP + SIDE, side, rest))
        return jnp.where(k < direct, piece_at, (1 - even) * SKIP + UP + k - direct)

    def wy_copy(j, k):
        r = piece(direct_piece(k))
        return remote(
            w_hbm.at[r],
            weight.at[dp, r],
            wy_send.at[j - 1],
            wy_recv.at[j - 1, k],
            sp,
            ((y + j) % chips) * 2 + core,
        )

    def wz_copy(j, k, down=True):
        shard = ((y - j + chips) % chips) * 2 + core
        r = piece(direct_piece(k))
        to = lax.rem(sp + n_sp - 2, n_sp) if down else lax.rem(sp + 2, n_sp)
        return remote(
            weight.at[shard, r],
            weight.at[shard, r],
            (wz_send if down else wu_send).at[j - 1],
            wz_recv.at[j - 1],
            to,
            dp,
        )

    def wz_each(j, k, do):
        @pl.when(g > 0)
        def _():
            do(wz_copy(j, k))

        if k < UP:

            @pl.when(g == n_groups - 2)
            def _():
                do(wz_copy(j, k, down=False))

    def wf_copy(j, k):
        shard = ((y - j + chips) % chips) * 2 + core
        r = piece(k + SKIP + SIDE)
        return remote(
            weight.at[shard, r],
            weight.at[shard, r],
            wf_send.at[j - 1],
            wf_recv.at[j - 1],
            lax.rem(sp + n_sp - 2, n_sp),
            dp,
        )

    def wx_copy(j, k):
        shard = ((y - j + chips) % chips) * 2 + core
        r = piece(direct_piece(k))
        return remote(
            weight.at[shard, r],
            weight.at[shard, r],
            wx_send.at[j - 1],
            wx_recv.at[j - 1],
            mate,
            dp,
        )

    def wd_copy(j, r):
        shard = ((y - j + chips) % chips) * 2 + core
        return remote(
            weight.at[shard, piece(r)],
            weight.at[shard, piece(r)],
            wd_send.at[j - 1],
            wd_recv.at[j - 1],
            sp,
            twin,
        )

    def mem_cross(at):
        return remote(
            cast.at[pl.ds(half * (1 - m), half)],
            mem_in.at[at],
            mem_send.at[0],
            cross_recv.at[0],
            mate,
            dp,
        )

    def norm_cross(at):
        return remote(
            norm_ref.at[pl.ds(half * (1 - m), half)],
            norm_in.at[at],
            mem_send.at[1],
            cross_recv.at[1],
            mate,
            dp,
        )

    def mem_down(d):
        to = lax.rem(sp + n_sp - 2 * d, n_sp)
        return [
            remote(cast.at[mine], mem_in.at[sp], down_send.at[0, d - 1], mem_recv.at[g], to, dp),
            remote(norm_ref.at[mine], norm_in.at[sp], down_send.at[1, d - 1], norm_recv.at[g], to, dp),
        ]

    def mem_relay(d):
        to = lax.rem(sp + n_sp - 2 * d, n_sp)
        return [
            remote(
                mem_in.at[mate], mem_in.at[mate], down_send.at[2, d - 1], mem_recv.at[g], to, dp
            ),
            remote(
                norm_in.at[mate], norm_in.at[mate], down_send.at[3, d - 1], norm_recv.at[g], to, dp
            ),
        ]

    for k in range(2):
        for j in range(1, chips):
            wy_copy(j, k).start()
    for d in range(1, n_sp):
        for copy in gate_copy(d):
            copy.start()
    mem_cross(sp).start()
    norm_cross(sp).start()

    @pl.loop(0, chunks)
    def _(c):
        x_copy(0, c).start()
        x_copy(1, c).start()

    @pl.loop(2, direct)
    def _(k):
        for j in range(1, chips):
            wy_copy(j, k).start()

    @pl.when(g == n_groups - 1)
    def _():
        for k in range(direct, direct + SKIP - UP):
            for j in range(1, chips):
                wy_copy(j, k).start()

    @pl.loop(0, chunks)
    def _(c):
        x_copy(2, c).start()

    own_copy().start()
    for d in range(1, n_groups):

        @pl.when(g >= d)
        def _():
            for copy in mem_down(d):
                copy.start()

    @pl.when(g == 0)
    def _():
        st_in[...] = jnp.zeros(st_in.shape, bf16)

    mem_in[sp] = cast[mine]
    norm_in[sp] = norm_ref[mine]
    for i in range(n_groups):

        @pl.when(i < g)
        def _():
            mem_in[2 * i : 2 * i + 2] = jnp.zeros((2, half, heads, channels, width), bf16)
            norm_in[2 * i : 2 * i + 2] = jnp.zeros((2, half, heads, width), f32)

    mem_cross(mate).wait_recv()
    norm_cross(mate).wait_recv()
    for d in range(1, n_groups):

        @pl.when(g >= d)
        def _():
            for copy in mem_relay(d):
                copy.start()

    local[0].wait()
    local[1].wait()
    arrived(igr.at[pl.ds(0, n_sp - 1)], gate_recv.at[0])
    arrived(fgr.at[pl.ds(0, n_sp - 1)], gate_recv.at[1])

    lane = lax.broadcasted_iota(jnp.int32, (n_groups * items, span), 1)

    def whole(ref):
        return jnp.concatenate(
            [
                jnp.concatenate(
                    [
                        ref[2 * i].astype(f32).reshape(items, tokens),
                        ref[2 * i + 1].astype(f32).reshape(items, tokens),
                    ],
                    axis=1,
                )
                for i in range(n_groups)
            ],
            axis=0,
        )

    gate_in = whole(igr)
    pre = whole(fgr)
    total = jnp.minimum(pre, 0.0) - jnp.log1p(jnp.exp(-jnp.abs(pre)))
    step = 1
    while step < span:
        total = total + jnp.where(lane >= step, pltpu.roll(total, step, 1), 0.0)
        step *= 2
    base = jnp.zeros((items, 1), f32)
    parts = []
    for i in range(n_groups):
        part = total[i * items : (i + 1) * items]
        parts.append(gate_in[i * items : (i + 1) * items] - (part + base))
        base = base + part[:, span - 1 : span]
    offset = jnp.concatenate(parts, axis=0)
    peak = offset
    step = 1
    while step < span:
        peak = jnp.maximum(peak, jnp.where(lane >= step, pltpu.roll(peak, step, 1), FILL))
        step *= 2
    local[7].wait()
    local[8].wait()
    eye = lax.broadcasted_iota(jnp.int32, (heads, heads), 0) == lax.broadcasted_iota(
        jnp.int32, (heads, heads), 1
    )
    level = jnp.concatenate(
        [
            jnp.sum(
                jnp.where(eye, level_ref[pl.ds(half * m + i, 1), :], 0.0), axis=1, keepdims=True
            )
            for i in range(half)
        ],
        axis=0,
    )
    level = jnp.broadcast_to(level, (items, span))
    for i in range(n_groups):
        part = peak[i * items : (i + 1) * items]
        starts[i] = level
        offs[i] = offset[i * items : (i + 1) * items]
        peaks[i] = jnp.maximum(part, level)
        level = jnp.maximum(level, jnp.broadcast_to(part[:, span - 1 : span], part.shape))
    starts[n_groups] = level
    first, last = starts[g], starts[g + 1]
    into[...] = jnp.exp(starts[0] - last)
    upon[...] = jnp.exp(starts[0] - first)
    mine_off = offs[g]
    off_g[...] = mine_off
    wrow[...] = jnp.exp(mine_off - last)
    arow[...] = jnp.exp(first - last)
    srow[...] = first
    for copy in local[2:5]:
        copy.wait()

    w_row = lax.broadcasted_iota(jnp.int32, (16, width), 0)
    tail_row = lax.broadcasted_iota(jnp.int32, (TAIL, width), 0)

    def grow(c):
        s, h = c // per_seq, (c % per_seq) * PER
        arrived(xk.at[s, pl.ds(h, PER)], x_recv.at[0, c])
        for p in range(PER):
            key, value = xk[s, h + p], xv[s, h + p]
            w = wrow[pl.ds(c * PER + p, 1), :]
            scaled = (jnp.transpose(key.astype(f32)) * w).astype(bf16)
            grown[c, p, :width] = jnp.dot(scaled, value, preferred_element_type=f32)
            start = into[pl.ds(c * PER + p, 1), :]
            for i in range(2):
                whole_ref[i * channels : (i + 1) * channels] = mem_in[2 * g + i, s, h + p].astype(
                    f32
                )
            rows_here = pl.ds(pl.multiple_of(g * 2 * channels, 2 * channels), 2 * channels)
            grown[c, p, rows_here] += whole_ref[0 : 2 * channels] * start
            high = w.astype(bf16).astype(f32)
            both = jnp.where(w_row == 0, high, jnp.where(w_row == 1, w - high, 0.0))
            norm = jnp.dot(both.astype(bf16), key, preferred_element_type=f32)
            norm = norm[0:1] + norm[1:2]
            for i in range(2):
                norm = norm + norm_in[2 * g + i, s, pl.ds(h + p, 1), :] * start
            grown[c, p, width:] = jnp.where(tail_row == 0, norm, 0.0)

    def st_copy(c, p):
        return remote(
            st_out.at[c, p],
            st_in.at[c, p],
            st_send.at[0],
            st_recv.at[c, p],
            lax.rem(sp + 2, n_sp),
            dp,
        )

    def initial(s, h):
        if channels % 16 == 0:
            return mem_in[:, s, h].reshape(width, width).astype(f32)
        for d in range(n_sp):
            whole_ref[d * channels : (d + 1) * channels] = mem_in[d, s, h].astype(f32)
        return whole_ref[...]

    def initial_arrived():
        for i in range(1, n_groups):

            @pl.when(i > g)
            def _():
                arrived(mem_in.at[pl.ds(2 * i, 2)], mem_recv.at[i])
                arrived(norm_in.at[pl.ds(2 * i, 2)], norm_recv.at[i])

        norm = norm_in[0].reshape(items, width)
        for d in range(1, n_sp):
            norm = norm + norm_in[d].reshape(items, width)
        norm_out[...] = norm

    def chain(c):
        for p in range(PER):

            @pl.when(g > 0)
            def _():
                st_copy(c, p).wait_recv()

            @pl.when(g < n_groups - 1)
            def _():
                a = arow[pl.ds(c * PER + p, 1), :]
                st_out[c, p] = (st_in[c, p].astype(f32) * a + grown[c, p]).astype(bf16)
                st_copy(c, p).start()

    def back_copy(c):
        s, h = c // per_seq, (c % per_seq) * PER
        lanes = pl.ds(pl.multiple_of(h * width, PER * width), PER * width)
        return remote(
            back.at[s, :, lanes],
            act.at[half * m + s, :, lanes],
            back_send.at[0],
            back_recv.at[s],
            mate,
            dp,
        )

    t_row = lax.broadcasted_iota(jnp.int32, (span, span), 0)
    s_col = lax.broadcasted_iota(jnp.int32, (span, span), 1)
    causal = s_col <= t_row
    ones = jnp.ones((span, width), bf16)

    def emit(c):
        x_copy(2, c).wait_recv()
        s, h = c // per_seq, (c % per_seq) * PER
        for p in range(PER):
            i = c * PER + p
            query, key, value = xq[s, h + p], xk[s, h + p], xv[s, h + p]
            start = upon[pl.ds(i, 1), :]
            memory = (
                st_in[c, p, :width].astype(f32) + initial(s, h + p) * start
            ).astype(bf16)
            norm = st_in[c, p, width:].astype(f32)[0:1] + norm_out[pl.ds(i, 1), :] * start
            norm = jnp.broadcast_to(norm, (width, width)).astype(bf16)
            raw = lax.dot_general(
                query,
                jnp.concatenate([key, norm], axis=0),
                (((1,), (1,)), ((), ())),
                preferred_element_type=f32,
            )
            column = pcol[i]
            gap = jnp.where(causal, off_g[pl.ds(i, 1), :] - column, FILL)
            scores = (raw[:, :span] * factor * jnp.exp(gap)).astype(bf16)
            weigh = jnp.exp(srow[pl.ds(i, 1), :] - column) * factor
            both = jnp.dot(
                scores, jnp.concatenate([value, ones], axis=1), preferred_element_type=f32
            )
            num = both[:, :width] + weigh * jnp.dot(query, memory, preferred_element_type=f32)
            den = both[:, width:] + weigh * raw[:, span:]
            hidden = (num / jnp.maximum(jnp.abs(den), 1.0)).astype(bf16)
            normed = (hidden.astype(f32) * gain_ref[pl.ds(h + p, 1), :]).astype(bf16)
            top, low = normed[:tokens], normed[tokens:]
            lanes = pl.ds(pl.multiple_of((h + p) * width, width), width)
            act[half * m + s, :, lanes] = jnp.where(m == 0, top, low)
            back[s, :, lanes] = jnp.where(m == 0, low, top)
        back_copy(c).start()

    columns_each = weight.shape[2]
    tile = min(1024, columns_each)
    tiles = columns_each // tile

    def project(which, first, last):
        picked = [base + s for s in which for base in (0, half)]
        left = jnp.concatenate([act[i] for i in picked], axis=0)

        for n in range(first, last):
            j, b = n // tiles, n % tiles
            shard = ((y + j // 2) % chips) * 2 + (core + j) % 2
            at = pl.ds(b * tile, tile)
            product = jnp.dot(left, weight[shard, :, at], preferred_element_type=f32).astype(bf16)
            to = pl.ds(pl.multiple_of(shard * columns_each + b * tile, tile), tile)
            for n_row, i in enumerate(picked):
                out_ref[i, :, to] = product[n_row * tokens : (n_row + 1) * tokens]

    def own_here():
        local[9].wait()
        own_copy().wait()

    def returned(s):
        arrived(act.at[s], back_recv.at[s])
    out_slot = jnp.maximum(chunks, HOP * g)
    slots = max(
        chunks + max(chunks, HOP * (n_groups - 1)),
        REST[-1] + 1,
        WHEN_SKIP + 1,
    )

    def pass_on(j, k):
        wy_copy(j, k).wait_recv()
        wd_copy(j, direct_piece(k)).start()

    def pass_rest(k):
        for j in range(1, chips):
            pass_on(j, k)
            if k < SKIP + 2 * SIDE:

                @pl.when(g == 1)
                def _():
                    wf_copy(j, k).start()

    def pass_first():
        for j in range(1, chips):
            arrived(weight.at[0, pl.ds(0, SIDE * rows), :], wf_recv.at[j - 1])
            for k in range(SIDE):
                wd_copy(j, 2 * SKIP + 2 * SIDE + k).start()

    def pass_skip(count):
        for j in range(1, chips):
            arrived(weight.at[0, pl.ds(0, count * rows), :], wz_recv.at[j - 1])
            for k in range(count):
                wd_copy(j, (1 - even) * SKIP + k).start()

    def pass_side():
        for j in range(1, chips):
            arrived(weight.at[0, pl.ds(0, SIDE * rows), :], wx_recv.at[j - 1])
            for k in range(SIDE):
                wd_copy(j, 2 * SKIP + m * SIDE + k).start()

    @pl.loop(0, slots)
    def _(t):
        @pl.when(t < chunks)
        def _():
            grow(t)

        for k in range(SKIP + SIDE):

            @pl.when(t == jnp.where(g == 0, LATE[k], WHEN[k]))
            def _():
                for j in range(1, chips):
                    pass_on(j, k)
                    if k < SKIP:
                        wz_each(j, k, lambda copy: copy.start())
                    else:

                        @pl.when(g > 0)
                        def _():
                            wx_copy(j, k).start()

        for k in range(SKIP + SIDE, SKIP + SIDE + len(REST)):

            @pl.when((g == n_groups - 1) & (t == REST[k - SKIP - SIDE]))
            def _():
                pass_rest(k)

        @pl.when((g == n_groups - 1) & (t == WHEN_SKIP))
        def _():
            pass_skip(UP)

        c = t - HOP * g

        @pl.when((c >= 0) & (c < chunks))
        def _():
            chain(c)

        @pl.when(t == 1)
        def _():
            columns = jnp.transpose(peaks[g])
            for i in range(items):
                pcol[i] = jnp.broadcast_to(columns[:, i : i + 1], (span, span))

        @pl.when(t == out_slot)
        def _():
            initial_arrived()

        o = t - out_slot

        @pl.when((o >= 0) & (o < chunks))
        def _():
            emit(o)

    def left_all(ref, sem):
        pltpu.make_async_copy(ref, ref, sem).wait()

    def sent_early():
        left_all(igr.at[pl.ds(0, n_sp - 1)], gate_send.at[0])
        left_all(fgr.at[pl.ds(0, n_sp - 1)], gate_send.at[1])
        for kind, ref in enumerate((xk, xv, xq)):
            left_all(ref.at[:, :, pl.ds(0, tokens), :], x_send.at[kind])
        mem_cross(sp).wait_send()
        norm_cross(sp).wait_send()
        for d in range(1, n_groups):

            @pl.when(g >= d)
            def _():
                for copy in mem_down(d) + mem_relay(d):
                    copy.wait_send()

        left_all(back, back_send.at[0])

        @pl.when(g < n_groups - 1)
        def _():
            left_all(st_out, st_send.at[0])

        for j in range(1, chips):

            @pl.when(g > 0)
            def _():
                left_all(weight.at[0, pl.ds(0, SKIP * rows), :], wz_send.at[j - 1])
                left_all(weight.at[0, pl.ds(0, SIDE * rows), :], wx_send.at[j - 1])

            @pl.when(g == n_groups - 2)
            def _():
                left_all(weight.at[0, pl.ds(0, UP * rows), :], wu_send.at[j - 1])

            @pl.when(g == 1)
            def _():
                left_all(weight.at[0, pl.ds(0, SIDE * rows), :], wf_send.at[j - 1])

    def sent_late():
        for j in range(1, chips):
            left_all(weight.at[0, pl.ds(0, direct * rows), :], wy_send.at[j - 1])
            left_all(weight.at[0], wd_send.at[j - 1])

            @pl.when(g == n_groups - 1)
            def _():
                left_all(weight.at[0, pl.ds(0, (SKIP - UP) * rows), :], wy_send.at[j - 1])

    def twin_arrived():
        for j in range(1, chips):
            arrived(weight.at[0], wd_recv.at[j - 1])

    every = list(range(half))
    near, far = 2 * tiles, n_dp * tiles

    first = SKIP + SIDE

    @pl.when(g < n_groups - 1)
    def _():
        for k in range(first, first + len(REST)):
            pass_rest(k)
        pass_skip(SKIP)

    for k in range(first + len(REST), direct - 1):
        pass_rest(k)

    @pl.when(g > 0)
    def _():
        pass_side()
        pass_rest(direct - 1)

    sent_early()
    own_here()
    for s in every:
        returned(s)

    project(every, 0, max(1, near // 2))

    @pl.when(g == 0)
    def _():
        pass_rest(direct - 1)
        pass_first()

    @pl.when(g == n_groups - 1)
    def _():
        for k in range(direct, direct + SKIP - UP):
            for j in range(1, chips):
                pass_on(j, k)

    project(every, max(1, near // 2), near)
    twin_arrived()
    project(every, near, far)
    sent_late()


def on_device(
    queries,
    keys,
    values,
    input_gate,
    forget_gate,
    start_memory,
    start_norm,
    start_level,
    head_gain,
    out_weight,
):
    seqs, heads, tokens, width = queries.shape
    n_sp, n_dp = lax.axis_size("sp"), lax.axis_size("dp")
    channels = start_memory.shape[2]
    mix, columns = out_weight.shape
    half = seqs // 2
    items = half * heads
    span = 2 * tokens
    groups = n_sp // 2
    chips = n_dp // 2
    chunks = items // PER
    direct = PIECES - SKIP - SIDE
    f32, bf16 = jnp.float32, jnp.bfloat16
    sizes = (n_sp, n_dp, seqs, heads, tokens, width, channels)
    operands = [
        pltpu.with_memory_space_constraint(array, pltpu.HBM)
        for array in (
            queries,
            keys,
            values,
            input_gate,
            forget_gate,
            out_weight,
            start_memory,
            start_norm,
            start_level,
            head_gain,
        )
    ]
    hbm_spec = pl.BlockSpec(memory_space=pltpu.HBM)
    vmem = pl.BlockSpec(memory_space=pltpu.VMEM)
    dma = pltpu.SemaphoreType.DMA
    return pl.pallas_call(
        lambda *refs: layer_kernel(sizes, *refs),
        out_shape=jax.ShapeDtypeStruct((seqs, tokens, n_dp * columns), bf16),
        in_specs=[hbm_spec] * len(operands),
        out_specs=vmem,
        scratch_shapes=[
            pltpu.VMEM((seqs, heads, channels, width), f32),
            pltpu.VMEM((seqs, heads, channels), f32),
            pltpu.VMEM((seqs, heads), f32),
            pltpu.VMEM((heads, width), f32),
            pltpu.VMEM((seqs, heads, width), f32),
            pltpu.VMEM((half, heads, span, width), bf16),
            pltpu.VMEM((half, heads, span, width), bf16),
            pltpu.VMEM((half, heads, span, width), bf16),
            pltpu.VMEM((n_sp, half, heads, tokens), bf16),
            pltpu.VMEM((n_sp, half, heads, tokens), bf16),
            pltpu.VMEM((seqs, heads, channels, width), bf16),
            pltpu.VMEM((n_sp, half, heads, channels, width), bf16),
            pltpu.VMEM((n_sp, half, heads, width), f32),
            pltpu.VMEM((items, width), f32),
            pltpu.VMEM((width, width), f32),
            pltpu.VMEM((groups, items, span), f32),
            pltpu.VMEM((groups, items, span), f32),
            pltpu.VMEM((groups + 1, items, span), f32),
            pltpu.VMEM((items, span), f32),
            pltpu.VMEM((items, span), f32),
            pltpu.VMEM((items, span), f32),
            pltpu.VMEM((items, span), f32),
            pltpu.VMEM((items, span), f32),
            pltpu.VMEM((items, span), f32),
            pltpu.VMEM((items, span, span), f32),
            pltpu.VMEM((chunks, PER, width + TAIL, width), f32),
            pltpu.VMEM((chunks, PER, width + TAIL, width), bf16),
            pltpu.VMEM((chunks, PER, width + TAIL, width), bf16),
            pltpu.VMEM((seqs, tokens, heads * width), bf16),
            pltpu.VMEM((half, tokens, heads * width), bf16),
            pltpu.VMEM((n_dp, mix, columns), bf16),
            dma((10,)),
            dma((2,)),
            dma((2,)),
            dma((3,)),
            dma((2, chunks)),
            dma((2,)),
            dma((2,)),
            dma((groups,)),
            dma((4, groups - 1)),
            dma((groups,)),
            dma((1,)),
            dma((chunks, PER)),
            dma((1,)),
            dma((half,)),
            dma((chips - 1,)),
            dma((chips - 1, direct + SKIP - UP)),
            dma((chips - 1,)),
            dma((chips - 1,)),
            dma((chips - 1,)),
            dma((chips - 1,)),
            dma((chips - 1,)),
            dma((chips - 1,)),
            dma((chips - 1,)),
            dma((chips - 1,)),
            dma((chips - 1,)),
            dma((1,)),
            dma((1,)),
        ],
        compiler_params=pltpu.CompilerParams(
            collective_id=0, has_side_effects=True, vmem_limit_bytes=40 * 1024 * 1024
        ),
        name="layer",
    )(*operands)


def solution(mesh):
    in_specs = (
        P("dp", None, "sp", None),
        P("dp", None, "sp", None),
        P("dp", None, "sp", None),
        P("dp", None, "sp"),
        P("dp", None, "sp"),
        P("dp", None, "sp", None),
        P("dp", None, "sp"),
        P("dp", None),
        P(),
        P(None, "dp"),
    )
    out_specs = P("dp", "sp", None)
    return jax.shard_map(
        on_device, mesh=mesh, in_specs=in_specs, out_specs=out_specs, check_vma=False
    )
```
